32 devices in a mesh: sp: 8 (over z, x), tp: 4 (over y, core).
Axes of the slice: x: 2, y: 2, z: 4, core: 2. Of those that a mesh axis runs over, the one named last changes fastest.
Arguments:
- layer_input: bfloat16 [1280, 4096], P('sp', 'tp'), may hold values from -24 to 24
- output_grad: bfloat16 [1280, 4096], P('sp', 'tp'), may hold values from -24 to 24
- query_weight: bfloat16 [4096, 2048], P(None, 'tp'), may hold values from -0.09375 to 0.09375
- key_weight: bfloat16 [4096, 1024], P(None, 'tp'), may hold values from -0.09375 to 0.09375
- value_weight: bfloat16 [4096, 1024], P(None, 'tp'), may hold values from -0.09375 to 0.09375
- out_weight: bfloat16 [2048, 4096], P('tp'), may hold values from -0.125 to 0.125
- sink_logit: float32 [16], P('tp'), may hold values from 3 to 7
Outputs:
- input_grad: bfloat16 [1280, 4096], P('sp', 'tp')
- query_weight_grad: float32 [4096, 2048], P('sp', 'tp')
- key_weight_grad: float32 [4096, 1024], P('sp', 'tp')
- value_weight_grad: float32 [4096, 1024], P('sp', 'tp')
- out_weight_grad: float32 [2048, 4096], P('tp', 'sp')
- sink_grad: float32 [16], P('tp')
The draws below stay inside these ranges and needn't reach their ends.
All inputs are finite; a program needn't handle non-finite values.
Results may differ from the reference program's by a relative error of at most 0.015.
Values may be sent and summed in bfloat16 or wider, within the bound.
A program may use at most 192 MiB of HBM per device.

```python
import jax
import jax.numpy as jnp
from jax import lax

D = 4096
HEADS = 16
KV_HEADS = 8
HEAD = 128
WINDOW = 128
TOK_DEV = 160
TOKENS = 1280


def draw_layer_input(key, part):
    key_normal = jax.random.fold_in(key, 11)
    key_pairing = jax.random.fold_in(key, 12)
    normal_part = jnp.clip(jax.random.normal(key_normal, (TOKENS, D), jnp.float32), -4.0, 4.0)
    blocks = TOKENS // TOK_DEV
    pairing = jax.random.permutation(key_pairing, blocks)
    row_block = jnp.arange(TOKENS, dtype=jnp.int32) // TOK_DEV
    col_block = jnp.arange(D, dtype=jnp.int32) * blocks // D
    spiked = pairing[row_block][:, None] == col_block[None, :]
    values = normal_part * jnp.where(spiked, 3.0, 1.0)
    return values.astype(jnp.bfloat16)


def strengthened(entries, own_key, source, target, parts, factor):
    owner, partner = [(jnp.arange(entries.shape[axis_at]) // (entries.shape[axis_at] // parts)).reshape([-1 if axis == axis_at else 1 for axis in range(entries.ndim)]) for axis_at in (source, target)]
    chosen = jax.random.permutation(own_key, parts)[partner]
    strong = (owner == chosen) | (owner == (partner + parts // 2) % parts)
    return jnp.where(strong, factor * entries, entries)


def block_levels(stream_key, shape, cuts, smallest, largest):
    def one(dim, shards_of):
        draws = jax.random.uniform(jax.random.fold_in(jax.random.fold_in(stream_key, 6), dim), (shards_of,), jnp.float32, smallest / len(cuts), largest / len(cuts))
        return jnp.repeat(jnp.exp(draws), shape[dim] // shards_of).reshape((-1,) + (1,) * (len(shape) - dim - 1))

    level = one(*cuts[0])
    for cut in cuts[1:]:
        level = level * one(*cut)
    return level


def scatter_about(key, shape, deviation, limit, pieces=(), kind=jnp.bfloat16):
    entries = jax.random.normal(key, shape, jnp.float32) * deviation
    if len(pieces) > 0:
        entries = block_levels(key, shape, pieces, -0.22, 0.18) * entries
    return jnp.clip(entries, min=-limit, max=limit).astype(kind)


def bell_draw_with(stream_key, shape, deviation, bound, pieces, heavy, kind=jnp.bfloat16):
    entries = deviation * jax.random.normal(stream_key, shape, jnp.float32)
    if pieces:
        entries = entries * block_levels(stream_key, shape, pieces, -0.22, 0.18)
    return jnp.clip(strengthened(entries, jax.random.fold_in(stream_key, 3), *heavy), -bound, bound).astype(kind)


def setup_inputs(seed: int = 0) -> dict:
    key_list = jax.random.split(jax.random.key(seed), 8)
    return {
        "layer_input": draw_layer_input(jax.random.fold_in(key_list[7], 71), 0),
        "output_grad": bell_draw_with(key_list[1], (TOKENS, D), 4.0, 24.0, ((0, 8), (1, 4)), (0, 1, 8, 2.0)),
        "query_weight": scatter_about(key_list[2], (D, HEADS * HEAD), D ** -0.5, 0.09375, ((1, 4),)),
        "key_weight": scatter_about(key_list[3], (D, KV_HEADS * HEAD), D ** -0.5, 0.09375, ((1, 4),)),
        "value_weight": scatter_about(key_list[4], (D, KV_HEADS * HEAD), D ** -0.5, 0.09375, ((1, 4),)),
        "out_weight": scatter_about(key_list[5], (HEADS * HEAD, D), (HEADS * HEAD) ** -0.5, 0.125, ((0, 4),)),
        "sink_logit": jnp.clip(3.0 + 4.0 * jax.random.uniform(key_list[6], (HEADS,), jnp.float32) ** block_levels(key_list[6], (HEADS,), ((0, 4),), -0.2, 0.2), 3.0, 7.0),
    }


masked_score = -1e30


def reference(layer_input, output_grad, query_weight, key_weight, value_weight, out_weight, sink_logit):
    seq_len = layer_input.shape[0]
    group_size = HEADS // KV_HEADS
    scaling = HEAD ** -0.5
    block_count = seq_len // WINDOW
    queries = jnp.dot(layer_input, query_weight, preferred_element_type=jnp.float32).astype(jnp.bfloat16)
    queries = queries.reshape(seq_len, KV_HEADS, group_size, HEAD)
    key_rows = jnp.dot(layer_input, key_weight, preferred_element_type=jnp.float32).astype(jnp.bfloat16)
    key_rows = key_rows.reshape(seq_len, KV_HEADS, HEAD)
    value_rows = jnp.dot(layer_input, value_weight, preferred_element_type=jnp.float32).astype(jnp.bfloat16)
    value_rows = value_rows.reshape(seq_len, KV_HEADS, HEAD)
    out_rows_grad = jnp.dot(output_grad, out_weight.T, preferred_element_type=jnp.float32).astype(jnp.bfloat16)
    out_rows_grad = out_rows_grad.reshape(seq_len, KV_HEADS, group_size, HEAD)
    sink_column = sink_logit.astype(jnp.float32).reshape(KV_HEADS, group_size)[:, :, None]
    edge_three = ((WINDOW, WINDOW), (0, 0), (0, 0))
    edge_four = ((WINDOW, WINDOW), (0, 0), (0, 0), (0, 0))
    padded_keys = jnp.pad(key_rows, edge_three)
    padded_values = jnp.pad(value_rows, edge_three)

    def forward_block(block):
        offset = block * WINDOW
        query_block = lax.dynamic_slice_in_dim(queries, offset, WINDOW, 0).astype(jnp.float32)
        grad_block = lax.dynamic_slice_in_dim(out_rows_grad, offset, WINDOW, 0).astype(jnp.float32)
        key_band = lax.dynamic_slice_in_dim(padded_keys, offset, 3 * WINDOW, 0).astype(jnp.float32)
        value_band = lax.dynamic_slice_in_dim(padded_values, offset, 3 * WINDOW, 0).astype(jnp.float32)
        query_pos = offset + jnp.arange(WINDOW, dtype=jnp.int32)
        key_pos = offset - WINDOW + jnp.arange(3 * WINDOW, dtype=jnp.int32)
        in_window = (jnp.abs(query_pos[:, None] - key_pos[None, :]) <= WINDOW) & (key_pos[None, :] >= 0) & (key_pos[None, :] < seq_len)
        scores = jnp.einsum("qkgd,skd->kgqs", query_block, key_band) * scaling
        scores = jnp.where(in_window[None, None], scores, masked_score)
        row_max = jnp.maximum(jnp.max(scores, axis=-1), sink_column)
        row_total = jnp.sum(jnp.exp(scores - row_max[..., None]), axis=-1) + jnp.exp(sink_column - row_max)
        log_total = row_max + jnp.log(row_total)
        soft_weights = jnp.exp(scores - log_total[..., None])
        soft_rounded = soft_weights.astype(jnp.bfloat16)
        attended = jnp.einsum("kgqs,skd->qkgd", soft_rounded.astype(jnp.float32), value_band).astype(jnp.bfloat16)
        row_dots = jnp.sum(grad_block * attended.astype(jnp.float32), axis=-1)
        dots_moved = row_dots.transpose(1, 2, 0)
        prob_grads = jnp.einsum("qkgd,skd->kgqs", grad_block, value_band)
        score_grads = (soft_weights * (prob_grads - dots_moved[..., None])).astype(jnp.bfloat16)
        query_grads = (jnp.einsum("kgqs,skd->qkgd", score_grads.astype(jnp.float32), key_band) * scaling).astype(jnp.bfloat16)
        sink_part = -jnp.sum(jnp.exp(sink_column - log_total) * dots_moved, axis=-1)
        return attended, log_total, row_dots, query_grads, sink_part

    attended, log_total, row_dots, query_grads, sink_parts = lax.map(forward_block, jnp.arange(block_count, dtype=jnp.int32))
    attended = attended.reshape(seq_len, HEADS * HEAD)
    log_total = log_total.transpose(0, 3, 1, 2).reshape(seq_len, KV_HEADS, group_size)
    row_dots = row_dots.reshape(seq_len, KV_HEADS, group_size)
    query_grads = query_grads.reshape(seq_len, HEADS * HEAD)
    sink_grad = jnp.sum(sink_parts, axis=0).reshape(HEADS)
    padded_queries = jnp.pad(queries, edge_four)
    padded_out_grad = jnp.pad(out_rows_grad, edge_four)
    padded_totals = jnp.pad(log_total, edge_three)
    padded_dots = jnp.pad(row_dots, edge_three)

    def key_block(block):
        offset = block * WINDOW
        key_own = lax.dynamic_slice_in_dim(key_rows, offset, WINDOW, 0).astype(jnp.float32)
        value_own = lax.dynamic_slice_in_dim(value_rows, offset, WINDOW, 0).astype(jnp.float32)
        query_band = lax.dynamic_slice_in_dim(padded_queries, offset, 3 * WINDOW, 0).astype(jnp.float32)
        grad_band = lax.dynamic_slice_in_dim(padded_out_grad, offset, 3 * WINDOW, 0).astype(jnp.float32)
        total_band = lax.dynamic_slice_in_dim(padded_totals, offset, 3 * WINDOW, 0).transpose(1, 2, 0)
        dots_band = lax.dynamic_slice_in_dim(padded_dots, offset, 3 * WINDOW, 0).transpose(1, 2, 0)
        query_pos = offset - WINDOW + jnp.arange(3 * WINDOW, dtype=jnp.int32)
        key_pos = offset + jnp.arange(WINDOW, dtype=jnp.int32)
        in_window = (jnp.abs(query_pos[:, None] - key_pos[None, :]) <= WINDOW) & (query_pos[:, None] >= 0) & (query_pos[:, None] < seq_len)
        scores = jnp.einsum("qkgd,skd->kgqs", query_band, key_own) * scaling
        scores = jnp.where(in_window[None, None], scores, masked_score)
        soft_weights = jnp.exp(scores - total_band[..., None])
        soft_rounded = soft_weights.astype(jnp.bfloat16)
        prob_grads = jnp.einsum("qkgd,skd->kgqs", grad_band, value_own)
        score_grads = (soft_weights * (prob_grads - dots_band[..., None])).astype(jnp.bfloat16)
        key_grads = (jnp.einsum("kgqs,qkgd->skd", score_grads.astype(jnp.float32), query_band) * scaling).astype(jnp.bfloat16)
        value_grads = jnp.einsum("kgqs,qkgd->skd", soft_rounded.astype(jnp.float32), grad_band).astype(jnp.bfloat16)
        return key_grads, value_grads

    key_grads, value_grads = lax.map(key_block, jnp.arange(block_count, dtype=jnp.int32))
    key_grads = key_grads.reshape(seq_len, KV_HEADS * HEAD)
    value_grads = value_grads.reshape(seq_len, KV_HEADS * HEAD)
    input_grad = (jnp.dot(query_grads, query_weight.T, preferred_element_type=jnp.float32)
                  + jnp.dot(key_grads, key_weight.T, preferred_element_type=jnp.float32)
                  + jnp.dot(value_grads, value_weight.T, preferred_element_type=jnp.float32)).astype(jnp.bfloat16)
    query_weight_grad = jnp.dot(layer_input.T, query_grads, preferred_element_type=jnp.float32)
    key_weight_grad = jnp.dot(layer_input.T, key_grads, preferred_element_type=jnp.float32)
    value_weight_grad = jnp.dot(layer_input.T, value_grads, preferred_element_type=jnp.float32)
    out_weight_grad = jnp.dot(attended.T, output_grad, preferred_element_type=jnp.float32)
    return (input_grad, query_weight_grad, key_weight_grad, value_weight_grad, out_weight_grad, sink_grad)
```

```python
import jax
import jax.numpy as jnp
from jax import lax
from jax.sharding import PartitionSpec as P

HEADS = 16
KV_HEADS = 8
HEAD = 128
WINDOW = 128


masked_score = -1e30


def extended(cells, sides, width):
    for axis, dim in sides:
        count = lax.axis_size(axis)
        ends = count - 1
        head = lax.slice_in_dim(cells, 0, width, axis=dim)
        tail = lax.slice_in_dim(cells, cells.shape[dim] - width, cells.shape[dim], axis=dim)
        cells = jnp.concatenate(
            [
                lax.ppermute(tail, axis, [(i, (i + 1) % count) for i in range(ends)]),
                cells,
                lax.ppermute(head, axis, [((i + 1) % count, i) for i in range(ends)]),
            ],
            axis=dim,
        )
    return cells


def passed_along(value, axis, steps):
    count = lax.axis_size(axis)
    initial, last = (max(0, -steps), min(count, count - steps))
    return lax.ppermute(value, axis, [(source, source + steps) for source in range(initial, last)])


def contract_rows(left, right):
    return lax.dot_general(
        left, right, (((0,), (0,)), ((), ())), preferred_element_type=jnp.float32
    )


def contract_cols(left, right):
    return lax.dot_general(
        left, right, (((1,), (1,)), ((), ())), preferred_element_type=jnp.float32
    )


def per_device(
    layer_input, output_grad, query_weight, key_weight, value_weight, out_weight, sink_logit
):
    whole_input, whole_grad = (
        lax.all_gather(layer_input, "tp", axis=1, tiled=True),
        lax.all_gather(output_grad, "tp", axis=1, tiled=True),
    )
    tok_rows = whole_input.shape[0]
    query_cols = query_weight.shape[1]
    key_cols = key_weight.shape[1]
    key_heads = key_cols // HEAD
    group_size = HEADS // KV_HEADS
    scaling = HEAD ** (-0.5)
    queries = jnp.dot(whole_input, query_weight, preferred_element_type=jnp.float32).astype(
        jnp.bfloat16
    )
    key_rows = jnp.dot(whole_input, key_weight, preferred_element_type=jnp.float32).astype(
        jnp.bfloat16
    )
    value_rows = jnp.dot(whole_input, value_weight, preferred_element_type=jnp.float32).astype(
        jnp.bfloat16
    )
    out_rows_grad = contract_cols(whole_grad, out_weight).astype(jnp.bfloat16)
    joined = jnp.concatenate([key_rows, value_rows], axis=1)
    band = extended(joined, (("sp", 0),), WINDOW)
    band_rows = band.shape[0]
    band_keys = band[:, :key_cols].reshape(band_rows, key_heads, HEAD)
    band_values = band[:, key_cols:].reshape(band_rows, key_heads, HEAD)
    shard_index = lax.axis_index("sp")
    seq_total = tok_rows * lax.axis_size("sp")
    query_pos = shard_index * tok_rows + jnp.arange(tok_rows, dtype=jnp.int32)
    key_pos = shard_index * tok_rows - WINDOW + jnp.arange(band_rows, dtype=jnp.int32)
    in_window = (
        (jnp.abs(query_pos[:, None] - key_pos[None, :]) <= WINDOW)
        & (key_pos[None, :] >= 0)
        & (key_pos[None, :] < seq_total)
    )
    query_heads = queries.reshape(tok_rows, key_heads, group_size, HEAD)
    grad_heads = out_rows_grad.reshape(tok_rows, key_heads, group_size, HEAD)
    scores = (
        jnp.einsum("qkgd,skd->kgqs", query_heads, band_keys, preferred_element_type=jnp.float32)
        * scaling
    )
    scores = jnp.where(in_window[None, None], scores, masked_score)
    sink_column = sink_logit.reshape(key_heads, group_size)[:, :, None]
    row_max = jnp.maximum(jnp.max(scores, axis=-1), sink_column)
    row_total = jnp.sum(jnp.exp(scores - row_max[..., None]), axis=-1) + jnp.exp(
        sink_column - row_max
    )
    log_total = row_max + jnp.log(row_total)
    soft_weights = jnp.exp(scores - log_total[..., None])
    soft_rounded = soft_weights.astype(jnp.bfloat16)
    attended = jnp.einsum(
        "kgqs,skd->qkgd", soft_rounded, band_values, preferred_element_type=jnp.float32
    ).astype(jnp.bfloat16)
    row_dots = jnp.sum(
        grad_heads.astype(jnp.float32) * attended.astype(jnp.float32), axis=-1
    ).transpose(1, 2, 0)
    prob_grads = jnp.einsum(
        "qkgd,skd->kgqs", grad_heads, band_values, preferred_element_type=jnp.float32
    )
    score_grads = (soft_weights * (prob_grads - row_dots[..., None])).astype(jnp.bfloat16)
    query_grads = (
        jnp.einsum("kgqs,skd->qkgd", score_grads, band_keys, preferred_element_type=jnp.float32)
        * scaling
    )
    query_grads = query_grads.astype(jnp.bfloat16).reshape(tok_rows, query_cols)
    band_key_grads = (
        jnp.einsum("kgqs,qkgd->skd", score_grads, query_heads, preferred_element_type=jnp.float32)
        * scaling
    )
    band_value_grads = jnp.einsum(
        "kgqs,qkgd->skd", soft_rounded, grad_heads, preferred_element_type=jnp.float32
    )
    band_grads = jnp.concatenate(
        [
            band_key_grads.reshape(band_rows, key_cols),
            band_value_grads.reshape(band_rows, key_cols),
        ],
        axis=1,
    )
    sink_part = -jnp.sum(jnp.exp(sink_column - log_total) * row_dots, axis=-1).reshape(-1)
    sink_grad = lax.psum(sink_part, "sp")
    attended_rows = attended.reshape(tok_rows, query_cols)
    input_block = lax.all_to_all(whole_input, "sp", 1, 0, tiled=True)
    grad_block = lax.all_to_all(whole_grad, "sp", 1, 0, tiled=True)
    early_rows = lax.all_gather(
        jnp.concatenate([query_grads, attended_rows], axis=1), "sp", axis=0, tiled=True
    )
    query_part = contract_rows(input_block, early_rows[:, :query_cols])
    out_part = contract_rows(early_rows[:, query_cols:], grad_block)
    returned_low = passed_along(band_grads[:WINDOW].astype(jnp.bfloat16), "sp", -1).astype(
        jnp.float32
    )
    returned_high = passed_along(
        band_grads[band_rows - WINDOW :].astype(jnp.bfloat16), "sp", 1
    ).astype(jnp.float32)
    own_rows = band_grads[WINDOW : WINDOW + tok_rows]
    own_rows = own_rows.at[tok_rows - WINDOW :].add(returned_low)
    own_rows = own_rows.at[:WINDOW].add(returned_high)
    key_grads = own_rows[:, :key_cols].astype(jnp.bfloat16)
    value_grads = own_rows[:, key_cols:].astype(jnp.bfloat16)
    late_rows = lax.all_gather(
        jnp.concatenate([key_grads, value_grads], axis=1), "sp", axis=0, tiled=True
    )
    key_part = contract_rows(input_block, late_rows[:, :key_cols])
    value_part = contract_rows(input_block, late_rows[:, key_cols:])
    partials = (
        contract_cols(query_grads, query_weight)
        + contract_cols(key_grads, key_weight)
        + contract_cols(value_grads, value_weight)
    )
    input_grad = lax.psum_scatter(
        partials.astype(jnp.bfloat16), "tp", scatter_dimension=1, tiled=True
    )
    return (input_grad, query_part, key_part, value_part, out_part, sink_grad)


def solution(mesh):
    placed = (
        P("sp", "tp"),
        P("sp", "tp"),
        P(None, "tp"),
        P(None, "tp"),
        P(None, "tp"),
        P("tp", None),
        P("tp"),
    )
    return jax.shard_map(
        per_device,
        mesh=mesh,
        in_specs=placed,
        out_specs=(
            P("sp", "tp"),
            P("sp", "tp"),
            P("sp", "tp"),
            P("sp", "tp"),
            P("tp", "sp"),
            P("tp"),
        ),
        check_vma=False,
    )
```

```python
import functools

import jax
import jax.numpy as jnp
from jax import lax
from jax.experimental import pallas as pl
from jax.experimental.pallas import tpu as pltpu
from jax.sharding import PartitionSpec as P

HEADS = 16
KV_HEADS = 8
HEAD = 128
WINDOW = 128


masked_score = -1e30


def extended(cells, sides, width):
    for axis, dim in sides:
        count = lax.axis_size(axis)
        ends = count - 1
        head = lax.slice_in_dim(cells, 0, width, axis=dim)
        tail = lax.slice_in_dim(cells, cells.shape[dim] - width, cells.shape[dim], axis=dim)
        cells = jnp.concatenate(
            [
                lax.ppermute(tail, axis, [(i, (i + 1) % count) for i in range(ends)]),
                cells,
                lax.ppermute(head, axis, [((i + 1) % count, i) for i in range(ends)]),
            ],
            axis=dim,
        )
    return cells


def passed_along(value, axis, steps):
    count = lax.axis_size(axis)
    initial, last = (max(0, -steps), min(count, count - steps))
    return lax.ppermute(value, axis, [(source, source + steps) for source in range(initial, last)])


def contract_rows(left, right):
    return lax.dot_general(
        left, right, (((0,), (0,)), ((), ())), preferred_element_type=jnp.float32
    )


def contract_cols(left, right):
    return lax.dot_general(
        left, right, (((1,), (1,)), ((), ())), preferred_element_type=jnp.float32
    )


def per_device(
    layer_input, output_grad, query_weight, key_weight, value_weight, out_weight, sink_logit
):
    whole_input, whole_grad = (
        lax.all_gather(layer_input, "tp", axis=1, tiled=True),
        lax.all_gather(output_grad, "tp", axis=1, tiled=True),
    )
    tok_rows = whole_input.shape[0]
    query_cols = query_weight.shape[1]
    key_cols = key_weight.shape[1]
    key_heads = key_cols // HEAD
    group_size = HEADS // KV_HEADS
    scaling = HEAD ** (-0.5)
    queries = jnp.dot(whole_input, query_weight, preferred_element_type=jnp.float32).astype(
        jnp.bfloat16
    )
    key_rows = jnp.dot(whole_input, key_weight, preferred_element_type=jnp.float32).astype(
        jnp.bfloat16
    )
    value_rows = jnp.dot(whole_input, value_weight, preferred_element_type=jnp.float32).astype(
        jnp.bfloat16
    )
    out_rows_grad = contract_cols(whole_grad, out_weight).astype(jnp.bfloat16)
    joined = jnp.concatenate([key_rows, value_rows], axis=1)
    band = extended(joined, (("sp", 0),), WINDOW)
    band_rows = band.shape[0]
    band_keys = band[:, :key_cols].reshape(band_rows, key_heads, HEAD)
    band_values = band[:, key_cols:].reshape(band_rows, key_heads, HEAD)
    shard_index = lax.axis_index("sp")
    seq_total = tok_rows * lax.axis_size("sp")
    query_pos = shard_index * tok_rows + jnp.arange(tok_rows, dtype=jnp.int32)
    key_pos = shard_index * tok_rows - WINDOW + jnp.arange(band_rows, dtype=jnp.int32)
    in_window = (
        (jnp.abs(query_pos[:, None] - key_pos[None, :]) <= WINDOW)
        & (key_pos[None, :] >= 0)
        & (key_pos[None, :] < seq_total)
    )
    query_heads = queries.reshape(tok_rows, key_heads, group_size, HEAD)
    grad_heads = out_rows_grad.reshape(tok_rows, key_heads, group_size, HEAD)
    scores = (
        jnp.einsum("qkgd,skd->kgqs", query_heads, band_keys, preferred_element_type=jnp.float32)
        * scaling
    )
    scores = jnp.where(in_window[None, None], scores, masked_score)
    sink_column = sink_logit.reshape(key_heads, group_size)[:, :, None]
    row_max = jnp.maximum(jnp.max(scores, axis=-1), sink_column)
    row_total = jnp.sum(jnp.exp(scores - row_max[..., None]), axis=-1) + jnp.exp(
        sink_column - row_max
    )
    log_total = row_max + jnp.log(row_total)
    soft_weights = jnp.exp(scores - log_total[..., None])
    soft_rounded = soft_weights.astype(jnp.bfloat16)
    attended = jnp.einsum(
        "kgqs,skd->qkgd", soft_rounded, band_values, preferred_element_type=jnp.float32
    ).astype(jnp.bfloat16)
    row_dots = jnp.sum(
        grad_heads.astype(jnp.float32) * attended.astype(jnp.float32), axis=-1
    ).transpose(1, 2, 0)
    prob_grads = jnp.einsum(
        "qkgd,skd->kgqs", grad_heads, band_values, preferred_element_type=jnp.float32
    )
    score_grads = (soft_weights * (prob_grads - row_dots[..., None])).astype(jnp.bfloat16)
    query_grads = (
        jnp.einsum("kgqs,skd->qkgd", score_grads, band_keys, preferred_element_type=jnp.float32)
        * scaling
    )
    query_grads = query_grads.astype(jnp.bfloat16).reshape(tok_rows, query_cols)
    band_key_grads = (
        jnp.einsum("kgqs,qkgd->skd", score_grads, query_heads, preferred_element_type=jnp.float32)
        * scaling
    )
    band_value_grads = jnp.einsum(
        "kgqs,qkgd->skd", soft_rounded, grad_heads, preferred_element_type=jnp.float32
    )
    band_grads = jnp.concatenate(
        [
            band_key_grads.reshape(band_rows, key_cols),
            band_value_grads.reshape(band_rows, key_cols),
        ],
        axis=1,
    )
    sink_part = -jnp.sum(jnp.exp(sink_column - log_total) * row_dots, axis=-1).reshape(-1)
    sink_grad = lax.psum(sink_part, "sp")
    attended_rows = attended.reshape(tok_rows, query_cols)
    input_block = lax.all_to_all(whole_input, "sp", 1, 0, tiled=True)
    grad_block = lax.all_to_all(whole_grad, "sp", 1, 0, tiled=True)
    early_rows = lax.all_gather(
        jnp.concatenate([query_grads, attended_rows], axis=1), "sp", axis=0, tiled=True
    )
    query_part = contract_rows(input_block, early_rows[:, :query_cols])
    out_part = contract_rows(early_rows[:, query_cols:], grad_block)
    returned_low = passed_along(band_grads[:WINDOW].astype(jnp.bfloat16), "sp", -1).astype(
        jnp.float32
    )
    returned_high = passed_along(
        band_grads[band_rows - WINDOW :].astype(jnp.bfloat16), "sp", 1
    ).astype(jnp.float32)
    own_rows = band_grads[WINDOW : WINDOW + tok_rows]
    own_rows = own_rows.at[tok_rows - WINDOW :].add(returned_low)
    own_rows = own_rows.at[:WINDOW].add(returned_high)
    key_grads = own_rows[:, :key_cols].astype(jnp.bfloat16)
    value_grads = own_rows[:, key_cols:].astype(jnp.bfloat16)
    late_rows = lax.all_gather(
        jnp.concatenate([key_grads, value_grads], axis=1), "sp", axis=0, tiled=True
    )
    key_part = contract_rows(input_block, late_rows[:, :key_cols])
    value_part = contract_rows(input_block, late_rows[:, key_cols:])
    partials = (
        contract_cols(query_grads, query_weight)
        + contract_cols(key_grads, key_weight)
        + contract_cols(value_grads, value_weight)
    )
    input_grad = lax.psum_scatter(
        partials.astype(jnp.bfloat16), "tp", scatter_dimension=1, tiled=True
    )
    return (input_grad, query_part, key_part, value_part, out_part, sink_grad)


LANES = 128
MESH = pl.DeviceIdType.MESH
VMEM_BYTES = 60 * 1024 * 1024


def dot_nn(a, b):
    return jnp.dot(a, b, preferred_element_type=jnp.float32)


def layer_kernel(
    x_ref, g_ref, wq_hbm, wk_hbm, wv_hbm, wo_hbm, sink_ref,
    ig_ref, gq_ref, gk_ref, gv_ref, go_ref, sg_ref,
    wq, wk, wv, wo, xg, acc, qs, dos, band, bg, ret_out, ret_in,
    blk, acts_e, acts_l, part, rs_in, sinks,
    w_sem, own_sem, ag_send, ag_recv, halo_send, halo_recv, ret_send, ret_recv,
    a2a_send, a2a_recv, blk_send, blk_recv, up_sem, down_sem, cross_sem, acts_recv,
    rs_send, rs_recv, sink_send, sink_recv,
):
    bf16 = jnp.bfloat16
    count, tps = lax.axis_size("sp"), lax.axis_size("tp")
    depth = count // 2
    s, t = lax.axis_index("sp"), lax.axis_index("tp")
    z, x = s // 2, s % 2
    y, core = t // 2, t % 2
    partner = y * 2 + (1 - core)
    across = (1 - y) * 2 + core
    diag = (1 - y) * 2 + (1 - core)
    rows, feats = x_ref.shape
    q_cols, k_cols = wq.shape[1], wk.shape[1]
    block_cols = gq_ref.shape[0]
    per_slot = feats // block_cols
    key_heads = k_cols // HEAD
    group = q_cols // k_cols
    scaling = HEAD**-0.5

    def remote(src, dst, send, recv, dev_s, dev_t):
        return pltpu.make_async_remote_copy(
            src_ref=src, dst_ref=dst, send_sem=send, recv_sem=recv,
            device_id=(dev_s, dev_t), device_id_type=MESH,
        )

    weights = [
        pltpu.make_async_copy(src, dst, w_sem.at[i])
        for i, (src, dst) in enumerate(((wq_hbm, wq), (wk_hbm, wk), (wv_hbm, wv), (wo_hbm, wo)))
    ]
    for copy in weights:
        copy.start()
    own = [
        pltpu.make_async_copy(ref, xg.at[t, a], own_sem.at[a])
        for a, ref in enumerate((x_ref, g_ref))
    ]
    for copy in own:
        copy.start()

    barrier = pltpu.get_barrier_semaphore()
    for peer in (partner, across, diag):
        pl.semaphore_signal(barrier, inc=1, device_id=(s, peer), device_id_type=MESH)
    for d in range(1, count):
        pl.semaphore_signal(
            barrier, inc=1, device_id=((s + d) % count, t), device_id_type=MESH
        )
    pl.semaphore_wait(barrier, 3 + count - 1)

    sources = (x_ref, g_ref)
    to_across = [
        remote(sources[a], xg.at[t, a], ag_send.at[0, a], ag_recv.at[0, a], s, across)
        for a in range(2)
    ]
    to_partner = [
        remote(sources[a], xg.at[t, a], ag_send.at[1, a], ag_recv.at[1, a], s, partner)
        for a in range(2)
    ]
    relay = [
        remote(xg.at[across, a], xg.at[across, a], ag_send.at[2, a], ag_recv.at[2, a], s, partner)
        for a in range(2)
    ]
    for copy in to_across + to_partner:
        copy.start()

    def project_input(slot, first):
        cells = xg[slot, 0]
        span = pl.ds(pl.multiple_of(slot * feats, feats), feats)
        at = 0
        for w in (wq, wk, wv):
            cols = w.shape[1]
            term = dot_nn(cells, w[span, :])
            acc[:, at : at + cols] = term if first else acc[:, at : at + cols] + term
            at += cols

    def project_grad(slot, first):
        span = pl.ds(pl.multiple_of(slot * feats, feats), feats)
        term = contract_cols(xg[slot, 1], wo[:, span])
        lo = q_cols + 2 * k_cols
        acc[:, lo:] = term if first else acc[:, lo:] + term

    for copy in own + weights:
        copy.wait()
    project_input(t, True)
    project_grad(t, True)
    to_partner[0].wait_recv()
    project_input(partner, False)
    to_partner[1].wait_recv()
    project_grad(partner, False)
    to_across[0].wait_recv()
    relay[0].start()
    project_input(across, False)
    relay[0].wait_recv()
    project_input(diag, False)

    mid = pl.ds(WINDOW, rows)
    band[mid, :] = acc[:, q_cols : q_cols + 2 * k_cols].astype(bf16)
    qs[...] = acc[:, :q_cols].astype(bf16)
    has_prev, has_next = s > 0, s < count - 1
    prev, nxt = lax.rem(s + count - 1, count), lax.rem(s + 1, count)
    low, high = pl.ds(0, WINDOW), pl.ds(WINDOW + rows, WINDOW)
    tail_copy = remote(
        band.at[pl.ds(rows, WINDOW)], band.at[low], halo_send.at[0], halo_recv.at[0], nxt, t
    )
    head_copy = remote(
        band.at[pl.ds(WINDOW, WINDOW)], band.at[high], halo_send.at[1], halo_recv.at[1], prev, t
    )

    @pl.when(has_next)
    def _():
        tail_copy.start()

    @pl.when(has_prev)
    def _():
        head_copy.start()

    to_across[1].wait_recv()
    relay[1].start()
    project_grad(across, False)
    relay[1].wait_recv()
    project_grad(diag, False)
    dos[...] = acc[:, q_cols + 2 * k_cols :].astype(bf16)

    def a2a_source(j):
        lane = (j % per_slot) * block_cols + t * LANES
        return xg.at[j // per_slot, :, :, pl.ds(pl.multiple_of(lane, LANES), LANES)]

    own_block = pltpu.make_async_copy(a2a_source(s), blk.at[t, s], own_sem.at[2])
    own_block.start()
    a2a = []
    for d in range(1, count):
        j = (s + d) % count
        a2a.append(
            remote(a2a_source(j), blk.at[t, s], a2a_send.at[d], a2a_recv.at[d], j, t)
        )
        a2a[-1].start()

    @pl.when(jnp.logical_not(has_prev))
    def _():
        band[low, :] = jnp.zeros((WINDOW, 2 * k_cols), bf16)

    @pl.when(jnp.logical_not(has_next))
    def _():
        band[high, :] = jnp.zeros((WINDOW, 2 * k_cols), bf16)

    @pl.when(has_prev)
    def _():
        tail_copy.wait_recv()

    @pl.when(has_next)
    def _():
        head_copy.wait_recv()

    band_rows = rows + 2 * WINDOW
    q_at = lax.broadcasted_iota(jnp.int32, (rows, band_rows), 0)
    k_at = lax.broadcasted_iota(jnp.int32, (rows, band_rows), 1) - WINDOW
    k_pos = k_at + s * rows
    in_window = (
        (jnp.abs(q_at - k_at) <= WINDOW) & (k_pos >= 0) & (k_pos < rows * count)
    )
    lane_at = lax.broadcasted_iota(jnp.int32, (8, LANES), 1)
    sink_row = jnp.zeros((8, LANES), jnp.float32)
    for kh in range(key_heads):
        keys = band[:, kh * HEAD : (kh + 1) * HEAD]
        values = band[:, k_cols + kh * HEAD : k_cols + (kh + 1) * HEAD]
        key_sum = value_sum = None
        for g in range(group):
            h = kh * group + g
            cols = slice(h * HEAD, (h + 1) * HEAD)
            q, do = qs[:, cols], dos[:, cols]
            scores = jnp.where(in_window, contract_cols(q, keys) * scaling, masked_score)
            sink = sink_ref[0, h]
            top = jnp.maximum(jnp.max(scores, axis=1, keepdims=True), sink)
            e = jnp.exp(scores - top)
            sink_e = jnp.exp(sink - top)
            inverse = 1.0 / (jnp.sum(e, axis=1, keepdims=True) + sink_e)
            p = e * inverse
            p_low = p.astype(bf16)
            attended = dot_nn(p_low, values).astype(bf16)
            dots = jnp.sum(
                do.astype(jnp.float32) * attended.astype(jnp.float32), axis=1, keepdims=True
            )
            ds = (p * (contract_cols(do, values) - dots)).astype(bf16)
            acts_e[s, :, cols] = (dot_nn(ds, keys) * scaling).astype(bf16)
            acts_e[s, :, q_cols + h * HEAD : q_cols + (h + 1) * HEAD] = attended
            kg, vg = contract_rows(ds, q), contract_rows(p_low, do)
            key_sum = kg if g == 0 else key_sum + kg
            value_sum = vg if g == 0 else value_sum + vg
            total = -jnp.sum(sink_e * inverse * dots)
            sink_row = jnp.where(lane_at == h, total, sink_row)
        bg[:, kh * HEAD : (kh + 1) * HEAD] = key_sum * scaling
        bg[:, k_cols + kh * HEAD : k_cols + (kh + 1) * HEAD] = value_sum
    sinks[s] = sink_row
    ret_out[0] = bg[low, :].astype(bf16)
    ret_out[1] = bg[high, :].astype(bf16)
    to_prev = remote(ret_out.at[0], ret_in.at[0], ret_send.at[0], ret_recv.at[0], prev, t)
    to_next = remote(ret_out.at[1], ret_in.at[1], ret_send.at[1], ret_recv.at[1], nxt, t)

    @pl.when(has_prev)
    def _():
        to_prev.start()

    @pl.when(has_next)
    def _():
        to_next.start()

    acts = (acts_e, acts_l)
    has_up, has_down = z < depth - 1, z > 0
    up, down, other = (z + 1) % depth * 2 + x, (z + depth - 1) % depth * 2 + x, z * 2 + (1 - x)

    def acts_copy(a, block, sems, dev):
        ref = acts[a].at[block]
        return remote(ref, ref, sems.at[a, block], acts_recv.at[a, block], dev, t)

    def send_own(a):
        acts_copy(a, s, cross_sem, other).start()

        @pl.when(has_up)
        def _():
            acts_copy(a, s, up_sem, up).start()

        @pl.when(has_down)
        def _():
            acts_copy(a, s, down_sem, down).start()

    send_own(0)
    sink_copies = []
    for d in range(1, count):
        sink_copies.append(
            remote(
                sinks.at[s], sinks.at[s], sink_send.at[d], sink_recv.at[d], (s + d) % count, t
            )
        )
        sink_copies[-1].start()

    tail, head = pl.ds(WINDOW + rows - WINDOW, WINDOW), pl.ds(WINDOW, WINDOW)

    @pl.when(has_next)
    def _():
        to_prev.wait_recv()
        bg[tail, :] = bg[tail, :] + ret_in[0].astype(jnp.float32)

    @pl.when(has_prev)
    def _():
        to_next.wait_recv()
        bg[head, :] = bg[head, :] + ret_in[1].astype(jnp.float32)

    acts_l[s] = bg[mid, :].astype(bf16)
    send_own(1)

    qg = acts_e[s, :, :q_cols]
    kg, vg = acts_l[s, :, :k_cols], acts_l[s, :, k_cols:]

    def partial_for(slot):
        span = pl.ds(pl.multiple_of(slot * feats, feats), feats)
        return (
            contract_cols(qg, wq[span, :])
            + contract_cols(kg, wk[span, :])
            + contract_cols(vg, wv[span, :])
        ).astype(bf16)

    rs_copies = []
    for i, peer in enumerate((across, diag, partner)):
        part[i] = partial_for(peer)
        rs_copies.append(
            remote(part.at[i], rs_in.at[i], rs_send.at[i], rs_recv.at[i], s, peer)
        )
        rs_copies[-1].start()

    def forward(d):
        for a in range(2):
            lower, upper = (z + depth - d) % depth * 2 + x, (z + d) % depth * 2 + x

            @pl.when(z >= d)
            def _():
                acts_copy(a, lower, up_sem, up).wait_recv()
                acts_copy(a, lower, cross_sem, other).start()

                @pl.when(has_up)
                def _():
                    acts_copy(a, lower, up_sem, up).start()

            @pl.when(z + d < depth)
            def _():
                acts_copy(a, upper, down_sem, down).wait_recv()
                acts_copy(a, upper, cross_sem, other).start()

                @pl.when(has_down)
                def _():
                    acts_copy(a, upper, down_sem, down).start()

    def consume(block, first=False):
        early, late = acts_e[block], acts_l[block]
        right = jnp.concatenate([early[:, :q_cols], late], axis=1)
        left = jnp.concatenate([blk[i, block, 0] for i in range(tps)], axis=1)
        grads = jnp.concatenate([blk[i, block, 1] for i in range(tps)], axis=1)
        term = contract_rows(left, right)
        out_term = contract_rows(early[:, q_cols:], grads)
        pieces = (
            (gq_ref, term[:, :q_cols]),
            (gk_ref, term[:, q_cols : q_cols + k_cols]),
            (gv_ref, term[:, q_cols + k_cols :]),
            (go_ref, out_term),
        )
        for ref, value in pieces:
            ref[...] = value if first else ref[...] + value

    def consume_crossed(block_z):
        block = block_z * 2 + (1 - x)
        for a in range(2):
            acts_copy(a, block, cross_sem, other).wait_recv()
        consume(block)

    def consume_far(d):
        lower, upper = (z + depth - d) % depth, (z + d) % depth

        @pl.when(z >= d)
        def _():
            consume(lower * 2 + x)
            consume_crossed(lower)

        @pl.when(z + d < depth)
        def _():
            consume(upper * 2 + x)
            consume_crossed(upper)

    own_block.wait()
    for copy in a2a:
        copy.wait_recv()
    blk_across = remote(blk.at[t], blk.at[t], blk_send.at[0], blk_recv.at[0], s, across)
    blk_partner = remote(blk.at[t], blk.at[t], blk_send.at[1], blk_recv.at[1], s, partner)
    blk_relay = remote(blk.at[across], blk.at[across], blk_send.at[2], blk_recv.at[2], s, partner)
    blk_across.start()
    blk_partner.start()
    forward(1)
    mine = partial_for(t)
    blk_across.wait_recv()
    blk_relay.start()
    blk_partner.wait_recv()
    blk_relay.wait_recv()
    consume(s, True)
    forward(2)
    consume_crossed(z)
    for d in range(1, depth):
        if d + 2 < depth:
            forward(d + 2)
        consume_far(d)
    for copy in rs_copies:
        copy.wait_recv()
    total = mine.astype(jnp.float32)
    for i in range(3):
        total = total + rs_in[i].astype(jnp.float32)
    ig_ref[...] = total.astype(bf16)
    for copy in sink_copies:
        copy.wait_recv()
    sink_total = sinks[0]
    for i in range(1, count):
        sink_total = sink_total + sinks[i]
    sg_ref[...] = sink_total

    for copy in to_across + to_partner + relay + a2a + rs_copies + sink_copies:
        copy.wait_send()
    for copy in (blk_across, blk_partner, blk_relay):
        copy.wait_send()

    @pl.when(has_next)
    def _():
        tail_copy.wait_send()
        to_next.wait_send()

    @pl.when(has_prev)
    def _():
        head_copy.wait_send()
        to_prev.wait_send()

    for a in range(2):
        acts_copy(a, s, cross_sem, other).wait_send()

        @pl.when(has_up)
        def _():
            acts_copy(a, s, up_sem, up).wait_send()

        @pl.when(has_down)
        def _():
            acts_copy(a, s, down_sem, down).wait_send()

        for d in range(1, depth):
            lower, upper = (z + depth - d) % depth * 2 + x, (z + d) % depth * 2 + x

            @pl.when(z >= d)
            def _():
                acts_copy(a, lower, cross_sem, other).wait_send()

                @pl.when(has_up)
                def _():
                    acts_copy(a, lower, up_sem, up).wait_send()

            @pl.when(z + d < depth)
            def _():
                acts_copy(a, upper, cross_sem, other).wait_send()

                @pl.when(has_down)
                def _():
                    acts_copy(a, upper, down_sem, down).wait_send()


def fused_device(
    layer_input, output_grad, query_weight, key_weight, value_weight, out_weight, sink_logit
):
    bf16, f32 = jnp.bfloat16, jnp.float32
    count, tps = lax.axis_size("sp"), lax.axis_size("tp")
    rows, feats = layer_input.shape
    width = query_weight.shape[0]
    q_cols, k_cols = query_weight.shape[1], key_weight.shape[1]
    block_cols = width // count
    vmem = pl.BlockSpec(memory_space=pltpu.VMEM)
    hbm = pl.BlockSpec(memory_space=pl.ANY)
    dma = pltpu.SemaphoreType.DMA
    outs = pl.pallas_call(
        layer_kernel,
        out_shape=(
            jax.ShapeDtypeStruct((rows, feats), bf16),
            jax.ShapeDtypeStruct((block_cols, q_cols), f32),
            jax.ShapeDtypeStruct((block_cols, k_cols), f32),
            jax.ShapeDtypeStruct((block_cols, k_cols), f32),
            jax.ShapeDtypeStruct((q_cols, block_cols), f32),
            jax.ShapeDtypeStruct((8, LANES), f32),
        ),
        in_specs=[vmem, vmem, hbm, hbm, hbm, hbm, pl.BlockSpec(memory_space=pltpu.SMEM)],
        out_specs=(vmem,) * 6,
        scratch_shapes=[
            pltpu.VMEM(query_weight.shape, bf16),
            pltpu.VMEM(key_weight.shape, bf16),
            pltpu.VMEM(value_weight.shape, bf16),
            pltpu.VMEM(out_weight.shape, bf16),
            pltpu.VMEM((tps, 2, rows, feats), bf16),
            pltpu.VMEM((rows, 2 * q_cols + 2 * k_cols), f32),
            pltpu.VMEM((rows, q_cols), bf16),
            pltpu.VMEM((rows, q_cols), bf16),
            pltpu.VMEM((rows + 2 * WINDOW, 2 * k_cols), bf16),
            pltpu.VMEM((rows + 2 * WINDOW, 2 * k_cols), f32),
            pltpu.VMEM((2, WINDOW, 2 * k_cols), bf16),
            pltpu.VMEM((2, WINDOW, 2 * k_cols), bf16),
            pltpu.VMEM((tps, count, 2, rows, LANES), bf16),
            pltpu.VMEM((count, rows, 2 * q_cols), bf16),
            pltpu.VMEM((count, rows, 2 * k_cols), bf16),
            pltpu.VMEM((3, rows, feats), bf16),
            pltpu.VMEM((3, rows, feats), bf16),
            pltpu.VMEM((count, 8, LANES), f32),
            dma((4,)), dma((3,)), dma((3, 2)), dma((3, 2)),
            dma((2,)), dma((2,)), dma((2,)), dma((2,)),
            dma((count,)), dma((count,)), dma((3,)), dma((3,)),
            dma((2, count)), dma((2, count)), dma((2, count)), dma((2, count)),
            dma((3,)), dma((3,)), dma((count,)), dma((count,)),
        ],
        compiler_params=pltpu.CompilerParams(
            collective_id=0, has_side_effects=True, vmem_limit_bytes=VMEM_BYTES
        ),
        name="layer",
    )(
        layer_input, output_grad, query_weight, key_weight, value_weight, out_weight,
        sink_logit.reshape(1, -1),
    )
    return outs[:5] + (outs[5][0, : sink_logit.shape[0]],)


def fits_kernel(mesh, layer_width):
    count, tps = mesh.shape["sp"], mesh.shape["tp"]
    return tps == 4 and count % 8 == 0 and layer_width == count * tps * LANES


def solution(mesh):
    placed = (
        P("sp", "tp"),
        P("sp", "tp"),
        P(None, "tp"),
        P(None, "tp"),
        P(None, "tp"),
        P("tp", None),
        P("tp"),
    )

    def sharded(*arrays):
        width = arrays[0].shape[1]
        body = fused_device if fits_kernel(mesh, width) else per_device
        return jax.shard_map(
            body,
            mesh=mesh,
            in_specs=placed,
            out_specs=(
                P("sp", "tp"),
                P("sp", "tp"),
                P("sp", "tp"),
                P("sp", "tp"),
                P("tp", "sp"),
                P("tp"),
            ),
            check_vma=False,
        )(*arrays)

    return sharded
```

```python
import functools

import jax
import jax.numpy as jnp
from jax import lax
from jax.experimental import pallas as pl
from jax.experimental.pallas import tpu as pltpu
from jax.sharding import PartitionSpec as P

HEADS = 16
KV_HEADS = 8
HEAD = 128
WINDOW = 128


masked_score = -1e30


def extended(cells, sides, width):
    for axis, dim in sides:
        count = lax.axis_size(axis)
        ends = count - 1
        head = lax.slice_in_dim(cells, 0, width, axis=dim)
        tail = lax.slice_in_dim(cells, cells.shape[dim] - width, cells.shape[dim], axis=dim)
        cells = jnp.concatenate(
            [
                lax.ppermute(tail, axis, [(i, (i + 1) % count) for i in range(ends)]),
                cells,
                lax.ppermute(head, axis, [((i + 1) % count, i) for i in range(ends)]),
            ],
            axis=dim,
        )
    return cells


def passed_along(value, axis, steps):
    count = lax.axis_size(axis)
    initial, last = (max(0, -steps), min(count, count - steps))
    return lax.ppermute(value, axis, [(source, source + steps) for source in range(initial, last)])


def contract_rows(left, right):
    return lax.dot_general(
        left, right, (((0,), (0,)), ((), ())), preferred_element_type=jnp.float32
    )


def contract_cols(left, right):
    return lax.dot_general(
        left, right, (((1,), (1,)), ((), ())), preferred_element_type=jnp.float32
    )


def per_device(
    layer_input, output_grad, query_weight, key_weight, value_weight, out_weight, sink_logit
):
    whole_input, whole_grad = (
        lax.all_gather(layer_input, "tp", axis=1, tiled=True),
        lax.all_gather(output_grad, "tp", axis=1, tiled=True),
    )
    tok_rows = whole_input.shape[0]
    query_cols = query_weight.shape[1]
    key_cols = key_weight.shape[1]
    key_heads = key_cols // HEAD
    group_size = HEADS // KV_HEADS
    scaling = HEAD ** (-0.5)
    queries = jnp.dot(whole_input, query_weight, preferred_element_type=jnp.float32).astype(
        jnp.bfloat16
    )
    key_rows = jnp.dot(whole_input, key_weight, preferred_element_type=jnp.float32).astype(
        jnp.bfloat16
    )
    value_rows = jnp.dot(whole_input, value_weight, preferred_element_type=jnp.float32).astype(
        jnp.bfloat16
    )
    out_rows_grad = contract_cols(whole_grad, out_weight).astype(jnp.bfloat16)
    joined = jnp.concatenate([key_rows, value_rows], axis=1)
    band = extended(joined, (("sp", 0),), WINDOW)
    band_rows = band.shape[0]
    band_keys = band[:, :key_cols].reshape(band_rows, key_heads, HEAD)
    band_values = band[:, key_cols:].reshape(band_rows, key_heads, HEAD)
    shard_index = lax.axis_index("sp")
    seq_total = tok_rows * lax.axis_size("sp")
    query_pos = shard_index * tok_rows + jnp.arange(tok_rows, dtype=jnp.int32)
    key_pos = shard_index * tok_rows - WINDOW + jnp.arange(band_rows, dtype=jnp.int32)
    in_window = (
        (jnp.abs(query_pos[:, None] - key_pos[None, :]) <= WINDOW)
        & (key_pos[None, :] >= 0)
        & (key_pos[None, :] < seq_total)
    )
    query_heads = queries.reshape(tok_rows, key_heads, group_size, HEAD)
    grad_heads = out_rows_grad.reshape(tok_rows, key_heads, group_size, HEAD)
    scores = (
        jnp.einsum("qkgd,skd->kgqs", query_heads, band_keys, preferred_element_type=jnp.float32)
        * scaling
    )
    scores = jnp.where(in_window[None, None], scores, masked_score)
    sink_column = sink_logit.reshape(key_heads, group_size)[:, :, None]
    row_max = jnp.maximum(jnp.max(scores, axis=-1), sink_column)
    row_total = jnp.sum(jnp.exp(scores - row_max[..., None]), axis=-1) + jnp.exp(
        sink_column - row_max
    )
    log_total = row_max + jnp.log(row_total)
    soft_weights = jnp.exp(scores - log_total[..., None])
    soft_rounded = soft_weights.astype(jnp.bfloat16)
    attended = jnp.einsum(
        "kgqs,skd->qkgd", soft_rounded, band_values, preferred_element_type=jnp.float32
    ).astype(jnp.bfloat16)
    row_dots = jnp.sum(
        grad_heads.astype(jnp.float32) * attended.astype(jnp.float32), axis=-1
    ).transpose(1, 2, 0)
    prob_grads = jnp.einsum(
        "qkgd,skd->kgqs", grad_heads, band_values, preferred_element_type=jnp.float32
    )
    score_grads = (soft_weights * (prob_grads - row_dots[..., None])).astype(jnp.bfloat16)
    query_grads = (
        jnp.einsum("kgqs,skd->qkgd", score_grads, band_keys, preferred_element_type=jnp.float32)
        * scaling
    )
    query_grads = query_grads.astype(jnp.bfloat16).reshape(tok_rows, query_cols)
    band_key_grads = (
        jnp.einsum("kgqs,qkgd->skd", score_grads, query_heads, preferred_element_type=jnp.float32)
        * scaling
    )
    band_value_grads = jnp.einsum(
        "kgqs,qkgd->skd", soft_rounded, grad_heads, preferred_element_type=jnp.float32
    )
    band_grads = jnp.concatenate(
        [
            band_key_grads.reshape(band_rows, key_cols),
            band_value_grads.reshape(band_rows, key_cols),
        ],
        axis=1,
    )
    sink_part = -jnp.sum(jnp.exp(sink_column - log_total) * row_dots, axis=-1).reshape(-1)
    sink_grad = lax.psum(sink_part, "sp")
    attended_rows = attended.reshape(tok_rows, query_cols)
    input_block = lax.all_to_all(whole_input, "sp", 1, 0, tiled=True)
    grad_block = lax.all_to_all(whole_grad, "sp", 1, 0, tiled=True)
    early_rows = lax.all_gather(
        jnp.concatenate([query_grads, attended_rows], axis=1), "sp", axis=0, tiled=True
    )
    query_part = contract_rows(input_block, early_rows[:, :query_cols])
    out_part = contract_rows(early_rows[:, query_cols:], grad_block)
    returned_low = passed_along(band_grads[:WINDOW].astype(jnp.bfloat16), "sp", -1).astype(
        jnp.float32
    )
    returned_high = passed_along(
        band_grads[band_rows - WINDOW :].astype(jnp.bfloat16), "sp", 1
    ).astype(jnp.float32)
    own_rows = band_grads[WINDOW : WINDOW + tok_rows]
    own_rows = own_rows.at[tok_rows - WINDOW :].add(returned_low)
    own_rows = own_rows.at[:WINDOW].add(returned_high)
    key_grads = own_rows[:, :key_cols].astype(jnp.bfloat16)
    value_grads = own_rows[:, key_cols:].astype(jnp.bfloat16)
    late_rows = lax.all_gather(
        jnp.concatenate([key_grads, value_grads], axis=1), "sp", axis=0, tiled=True
    )
    key_part = contract_rows(input_block, late_rows[:, :key_cols])
    value_part = contract_rows(input_block, late_rows[:, key_cols:])
    partials = (
        contract_cols(query_grads, query_weight)
        + contract_cols(key_grads, key_weight)
        + contract_cols(value_grads, value_weight)
    )
    input_grad = lax.psum_scatter(
        partials.astype(jnp.bfloat16), "tp", scatter_dimension=1, tiled=True
    )
    return (input_grad, query_part, key_part, value_part, out_part, sink_grad)


LANES = 128
MESH = pl.DeviceIdType.MESH
VMEM_BYTES = 60 * 1024 * 1024


def dot_nn(a, b):
    return jnp.dot(a, b, preferred_element_type=jnp.float32)


def layer_kernel(
    x_ref, g_ref, wq_hbm, wk_hbm, wv_hbm, wo_hbm, sink_ref,
    ig_ref, gq_ref, gk_ref, gv_ref, go_ref, sg_ref,
    wq, wk, wv, wo, xg, acc, qs, dos, band, bg, ret_out, ret_in,
    blk, acts_e, acts_l, part, rs_in, sinks,
    w_sem, own_sem, ag_send, ag_recv, halo_send, halo_recv, ret_send, ret_recv,
    a2a_send, a2a_recv, blk_send, blk_recv, up_sem, down_sem, cross_sem, acts_recv,
    rs_send, rs_recv, sink_send, sink_recv,
):
    bf16 = jnp.bfloat16
    count, tps = lax.axis_size("sp"), lax.axis_size("tp")
    depth = count // 2
    s, t = lax.axis_index("sp"), lax.axis_index("tp")
    z, x = s // 2, s % 2
    y, core = t // 2, t % 2
    partner = y * 2 + (1 - core)
    across = (1 - y) * 2 + core
    diag = (1 - y) * 2 + (1 - core)
    rows, feats = x_ref.shape
    q_cols, k_cols = wq.shape[1], wk.shape[1]
    block_cols = gq_ref.shape[0]
    per_slot = feats // block_cols
    key_heads = k_cols // HEAD
    group = q_cols // k_cols
    scaling = HEAD**-0.5

    def remote(src, dst, send, recv, dev_s, dev_t):
        return pltpu.make_async_remote_copy(
            src_ref=src, dst_ref=dst, send_sem=send, recv_sem=recv,
            device_id=(dev_s, dev_t), device_id_type=MESH,
        )

    weights = [
        pltpu.make_async_copy(src, dst, w_sem.at[i])
        for i, (src, dst) in enumerate(((wq_hbm, wq), (wk_hbm, wk), (wv_hbm, wv), (wo_hbm, wo)))
    ]
    for copy in weights:
        copy.start()
    own = [
        pltpu.make_async_copy(ref, xg.at[t, a], own_sem.at[a])
        for a, ref in enumerate((x_ref, g_ref))
    ]
    for copy in own:
        copy.start()

    barrier = pltpu.get_barrier_semaphore()
    for peer in (partner, across, diag):
        pl.semaphore_signal(barrier, inc=1, device_id=(s, peer), device_id_type=MESH)
    for d in range(1, count):
        pl.semaphore_signal(
            barrier, inc=1, device_id=((s + d) % count, t), device_id_type=MESH
        )
    pl.semaphore_wait(barrier, 3 + count - 1)

    sources = (x_ref, g_ref)
    to_across = [
        remote(sources[a], xg.at[t, a], ag_send.at[0, a], ag_recv.at[0, a], s, across)
        for a in range(2)
    ]
    to_partner = [
        remote(sources[a], xg.at[t, a], ag_send.at[1, a], ag_recv.at[1, a], s, partner)
        for a in range(2)
    ]
    relay = [
        remote(xg.at[across, a], xg.at[across, a], ag_send.at[2, a], ag_recv.at[2, a], s, partner)
        for a in range(2)
    ]
    for copy in to_across + to_partner:
        copy.start()

    def project_input(slot, first):
        cells = xg[slot, 0]
        span = pl.ds(pl.multiple_of(slot * feats, feats), feats)
        at = 0
        for w in (wq, wk, wv):
            cols = w.shape[1]
            term = dot_nn(cells, w[span, :])
            acc[:, at : at + cols] = term if first else acc[:, at : at + cols] + term
            at += cols

    def project_grad(slot, first):
        span = pl.ds(pl.multiple_of(slot * feats, feats), feats)
        term = contract_cols(xg[slot, 1], wo[:, span])
        lo = q_cols + 2 * k_cols
        acc[:, lo:] = term if first else acc[:, lo:] + term

    for copy in own + weights:
        copy.wait()
    project_input(t, True)
    project_grad(t, True)
    to_partner[0].wait_recv()
    project_input(partner, False)
    to_partner[1].wait_recv()
    project_grad(partner, False)
    to_across[0].wait_recv()
    relay[0].start()
    project_input(across, False)
    relay[0].wait_recv()
    project_input(diag, False)

    mid = pl.ds(WINDOW, rows)
    band[mid, :] = acc[:, q_cols : q_cols + 2 * k_cols].astype(bf16)
    qs[...] = acc[:, :q_cols].astype(bf16)
    has_prev, has_next = s > 0, s < count - 1
    prev, nxt = lax.rem(s + count - 1, count), lax.rem(s + 1, count)
    low, high = pl.ds(0, WINDOW), pl.ds(WINDOW + rows, WINDOW)
    tail_copy = remote(
        band.at[pl.ds(rows, WINDOW)], band.at[low], halo_send.at[0], halo_recv.at[0], nxt, t
    )
    head_copy = remote(
        band.at[pl.ds(WINDOW, WINDOW)], band.at[high], halo_send.at[1], halo_recv.at[1], prev, t
    )

    @pl.when(has_next)
    def _():
        tail_copy.start()

    @pl.when(has_prev)
    def _():
        head_copy.start()

    own_blocks, a2a = [], []

    def columns(a, j):
        lane = (j % per_slot) * block_cols + t * LANES
        return xg.at[j // per_slot, a, :, pl.ds(pl.multiple_of(lane, LANES), LANES)]

    def send_columns(a):
        own_blocks.append(
            pltpu.make_async_copy(columns(a, s), blk.at[t, s, a], own_sem.at[2 + a])
        )
        own_blocks[-1].start()
        for d in range(1, count):
            j = (s + d) % count
            a2a.append(
                remote(
                    columns(a, j), blk.at[t, s, a], a2a_send.at[a, d], a2a_recv.at[a, d], j, t
                )
            )
            a2a[-1].start()

    send_columns(0)
    to_across[1].wait_recv()
    relay[1].start()
    project_grad(across, False)
    relay[1].wait_recv()
    project_grad(diag, False)
    dos[...] = acc[:, q_cols + 2 * k_cols :].astype(bf16)

    send_columns(1)

    @pl.when(jnp.logical_not(has_prev))
    def _():
        band[low, :] = jnp.zeros((WINDOW, 2 * k_cols), bf16)

    @pl.when(jnp.logical_not(has_next))
    def _():
        band[high, :] = jnp.zeros((WINDOW, 2 * k_cols), bf16)

    @pl.when(has_prev)
    def _():
        tail_copy.wait_recv()

    @pl.when(has_next)
    def _():
        head_copy.wait_recv()

    band_rows = rows + 2 * WINDOW
    q_at = lax.broadcasted_iota(jnp.int32, (rows, band_rows), 0)
    k_at = lax.broadcasted_iota(jnp.int32, (rows, band_rows), 1) - WINDOW
    k_pos = k_at + s * rows
    in_window = (
        (jnp.abs(q_at - k_at) <= WINDOW) & (k_pos >= 0) & (k_pos < rows * count)
    )
    lane_at = lax.broadcasted_iota(jnp.int32, (8, LANES), 1)
    sink_row = jnp.zeros((8, LANES), jnp.float32)
    for kh in range(key_heads):
        keys = band[:, kh * HEAD : (kh + 1) * HEAD]
        values = band[:, k_cols + kh * HEAD : k_cols + (kh + 1) * HEAD]
        key_sum = value_sum = None
        for g in range(group):
            h = kh * group + g
            cols = slice(h * HEAD, (h + 1) * HEAD)
            q, do = qs[:, cols], dos[:, cols]
            scores = jnp.where(in_window, contract_cols(q, keys) * scaling, masked_score)
            sink = sink_ref[0, h]
            top = jnp.maximum(jnp.max(scores, axis=1, keepdims=True), sink)
            e = jnp.exp(scores - top)
            sink_e = jnp.exp(sink - top)
            inverse = 1.0 / (jnp.sum(e, axis=1, keepdims=True) + sink_e)
            p = e * inverse
            p_low = p.astype(bf16)
            attended = dot_nn(p_low, values).astype(bf16)
            dots = jnp.sum(
                do.astype(jnp.float32) * attended.astype(jnp.float32), axis=1, keepdims=True
            )
            ds = (p * (contract_cols(do, values) - dots)).astype(bf16)
            acts_e[s, :, cols] = (dot_nn(ds, keys) * scaling).astype(bf16)
            acts_e[s, :, q_cols + h * HEAD : q_cols + (h + 1) * HEAD] = attended
            kg, vg = contract_rows(ds, q), contract_rows(p_low, do)
            key_sum = kg if g == 0 else key_sum + kg
            value_sum = vg if g == 0 else value_sum + vg
            total = -jnp.sum(sink_e * inverse * dots)
            sink_row = jnp.where(lane_at == h, total, sink_row)
        bg[:, kh * HEAD : (kh + 1) * HEAD] = key_sum * scaling
        bg[:, k_cols + kh * HEAD : k_cols + (kh + 1) * HEAD] = value_sum
    sinks[s] = sink_row
    ret_out[0] = bg[low, :].astype(bf16)
    ret_out[1] = bg[high, :].astype(bf16)
    to_prev = remote(ret_out.at[0], ret_in.at[0], ret_send.at[0], ret_recv.at[0], prev, t)
    to_next = remote(ret_out.at[1], ret_in.at[1], ret_send.at[1], ret_recv.at[1], nxt, t)

    @pl.when(has_prev)
    def _():
        to_prev.start()

    @pl.when(has_next)
    def _():
        to_next.start()

    acts = (acts_e, acts_l)
    has_up, has_down = z < depth - 1, z > 0
    up, down, other = (z + 1) % depth * 2 + x, (z + depth - 1) % depth * 2 + x, z * 2 + (1 - x)

    def acts_copy(a, block, sems, dev):
        ref = acts[a].at[block]
        return remote(ref, ref, sems.at[a, block], acts_recv.at[a, block], dev, t)

    def send_own(a):
        acts_copy(a, s, cross_sem, other).start()

        @pl.when(has_up)
        def _():
            acts_copy(a, s, up_sem, up).start()

        @pl.when(has_down)
        def _():
            acts_copy(a, s, down_sem, down).start()

    send_own(0)
    sink_copies = []
    for d in range(1, count):
        sink_copies.append(
            remote(
                sinks.at[s], sinks.at[s], sink_send.at[d], sink_recv.at[d], (s + d) % count, t
            )
        )
        sink_copies[-1].start()

    tail, head = pl.ds(WINDOW + rows - WINDOW, WINDOW), pl.ds(WINDOW, WINDOW)

    @pl.when(has_next)
    def _():
        to_prev.wait_recv()
        bg[tail, :] = bg[tail, :] + ret_in[0].astype(jnp.float32)

    @pl.when(has_prev)
    def _():
        to_next.wait_recv()
        bg[head, :] = bg[head, :] + ret_in[1].astype(jnp.float32)

    acts_l[s] = bg[mid, :].astype(bf16)
    send_own(1)

    for copy in own_blocks:
        copy.wait()
    for copy in a2a:
        copy.wait_recv()
    blk_across = remote(blk.at[t], blk.at[t], blk_send.at[0], blk_recv.at[0], s, across)
    blk_partner = remote(blk.at[t], blk.at[t], blk_send.at[1], blk_recv.at[1], s, partner)
    blk_relay = remote(blk.at[across], blk.at[across], blk_send.at[2], blk_recv.at[2], s, partner)
    blk_across.start()
    blk_partner.start()
    qg = acts_e[s, :, :q_cols]
    kg, vg = acts_l[s, :, :k_cols], acts_l[s, :, k_cols:]

    def partial_for(slot):
        span = pl.ds(pl.multiple_of(slot * feats, feats), feats)
        return (
            contract_cols(qg, wq[span, :])
            + contract_cols(kg, wk[span, :])
            + contract_cols(vg, wv[span, :])
        ).astype(bf16)

    rs_copies = []
    for i, peer in enumerate((across, diag, partner)):
        part[i] = partial_for(peer)
        rs_copies.append(
            remote(part.at[i], rs_in.at[i], rs_send.at[i], rs_recv.at[i], s, peer)
        )
        rs_copies[-1].start()

    def forward(d):
        for a in range(2):
            lower, upper = (z + depth - d) % depth * 2 + x, (z + d) % depth * 2 + x

            @pl.when(z >= d)
            def _():
                acts_copy(a, lower, up_sem, up).wait_recv()
                acts_copy(a, lower, cross_sem, other).start()

                @pl.when(has_up)
                def _():
                    acts_copy(a, lower, up_sem, up).start()

            @pl.when(z + d < depth)
            def _():
                acts_copy(a, upper, down_sem, down).wait_recv()
                acts_copy(a, upper, cross_sem, other).start()

                @pl.when(has_down)
                def _():
                    acts_copy(a, upper, down_sem, down).start()

    def consume(block, first=False):
        early, late = acts_e[block], acts_l[block]
        right = jnp.concatenate([early[:, :q_cols], late], axis=1)
        left = jnp.concatenate([blk[i, block, 0] for i in range(tps)], axis=1)
        grads = jnp.concatenate([blk[i, block, 1] for i in range(tps)], axis=1)
        term = contract_rows(left, right)
        out_term = contract_rows(early[:, q_cols:], grads)
        pieces = (
            (gq_ref, term[:, :q_cols]),
            (gk_ref, term[:, q_cols : q_cols + k_cols]),
            (gv_ref, term[:, q_cols + k_cols :]),
            (go_ref, out_term),
        )
        for ref, value in pieces:
            ref[...] = value if first else ref[...] + value

    def consume_crossed(block_z):
        block = block_z * 2 + (1 - x)
        for a in range(2):
            acts_copy(a, block, cross_sem, other).wait_recv()
        consume(block)

    def consume_far(d):
        lower, upper = (z + depth - d) % depth, (z + d) % depth

        @pl.when(z >= d)
        def _():
            consume(lower * 2 + x)
            consume_crossed(lower)

        @pl.when(z + d < depth)
        def _():
            consume(upper * 2 + x)
            consume_crossed(upper)

    mine = partial_for(t)
    forward(1)
    blk_across.wait_recv()
    blk_relay.start()
    for d in range(2, depth):
        forward(d)
    blk_partner.wait_recv()
    blk_relay.wait_recv()
    consume(s, True)
    consume_crossed(z)
    for d in range(1, depth):
        consume_far(d)
    for copy in rs_copies:
        copy.wait_recv()
    total = mine.astype(jnp.float32)
    for i in range(3):
        total = total + rs_in[i].astype(jnp.float32)
    ig_ref[...] = total.astype(bf16)
    for copy in sink_copies:
        copy.wait_recv()
    sink_total = sinks[0]
    for i in range(1, count):
        sink_total = sink_total + sinks[i]
    sg_ref[...] = sink_total

    for copy in to_across + to_partner + relay + a2a + rs_copies + sink_copies:
        copy.wait_send()
    for copy in (blk_across, blk_partner, blk_relay):
        copy.wait_send()

    @pl.when(has_next)
    def _():
        tail_copy.wait_send()
        to_next.wait_send()

    @pl.when(has_prev)
    def _():
        head_copy.wait_send()
        to_prev.wait_send()

    for a in range(2):
        acts_copy(a, s, cross_sem, other).wait_send()

        @pl.when(has_up)
        def _():
            acts_copy(a, s, up_sem, up).wait_send()

        @pl.when(has_down)
        def _():
            acts_copy(a, s, down_sem, down).wait_send()

        for d in range(1, depth):
            lower, upper = (z + depth - d) % depth * 2 + x, (z + d) % depth * 2 + x

            @pl.when(z >= d)
            def _():
                acts_copy(a, lower, cross_sem, other).wait_send()

                @pl.when(has_up)
                def _():
                    acts_copy(a, lower, up_sem, up).wait_send()

            @pl.when(z + d < depth)
            def _():
                acts_copy(a, upper, cross_sem, other).wait_send()

                @pl.when(has_down)
                def _():
                    acts_copy(a, upper, down_sem, down).wait_send()


def store_kernel(*refs):
    ins, sink_in, outs, sink_out = refs[:5], refs[5], refs[6:11], refs[11]
    held, in_sem, out_sem = refs[12:17], refs[17], refs[18]
    loads = [pltpu.make_async_copy(ins[i], held[i], in_sem.at[i]) for i in range(5)]
    stores = [pltpu.make_async_copy(held[i], outs[i], out_sem.at[i]) for i in range(5)]
    for load in loads:
        load.start()
    sink_out[...] = sink_in[0:1, : sink_out.shape[1]]
    for load, store in zip(loads, stores):
        load.wait()
        store.start()
    for store in stores:
        store.wait()


def fused_device(
    layer_input, output_grad, query_weight, key_weight, value_weight, out_weight, sink_logit
):
    bf16, f32 = jnp.bfloat16, jnp.float32
    count, tps = lax.axis_size("sp"), lax.axis_size("tp")
    rows, feats = layer_input.shape
    width = query_weight.shape[0]
    q_cols, k_cols = query_weight.shape[1], key_weight.shape[1]
    block_cols = width // count
    vmem = pl.BlockSpec(memory_space=pltpu.VMEM)
    hbm = pl.BlockSpec(memory_space=pl.ANY)
    dma = pltpu.SemaphoreType.DMA
    outs = pl.pallas_call(
        layer_kernel,
        out_shape=(
            jax.ShapeDtypeStruct((rows, feats), bf16),
            jax.ShapeDtypeStruct((block_cols, q_cols), f32),
            jax.ShapeDtypeStruct((block_cols, k_cols), f32),
            jax.ShapeDtypeStruct((block_cols, k_cols), f32),
            jax.ShapeDtypeStruct((q_cols, block_cols), f32),
            jax.ShapeDtypeStruct((8, LANES), f32),
        ),
        in_specs=[vmem, vmem, hbm, hbm, hbm, hbm, pl.BlockSpec(memory_space=pltpu.SMEM)],
        out_specs=(vmem,) * 6,
        scratch_shapes=[
            pltpu.VMEM(query_weight.shape, bf16),
            pltpu.VMEM(key_weight.shape, bf16),
            pltpu.VMEM(value_weight.shape, bf16),
            pltpu.VMEM(out_weight.shape, bf16),
            pltpu.VMEM((tps, 2, rows, feats), bf16),
            pltpu.VMEM((rows, 2 * q_cols + 2 * k_cols), f32),
            pltpu.VMEM((rows, q_cols), bf16),
            pltpu.VMEM((rows, q_cols), bf16),
            pltpu.VMEM((rows + 2 * WINDOW, 2 * k_cols), bf16),
            pltpu.VMEM((rows + 2 * WINDOW, 2 * k_cols), f32),
            pltpu.VMEM((2, WINDOW, 2 * k_cols), bf16),
            pltpu.VMEM((2, WINDOW, 2 * k_cols), bf16),
            pltpu.VMEM((tps, count, 2, rows, LANES), bf16),
            pltpu.VMEM((count, rows, 2 * q_cols), bf16),
            pltpu.VMEM((count, rows, 2 * k_cols), bf16),
            pltpu.VMEM((3, rows, feats), bf16),
            pltpu.VMEM((3, rows, feats), bf16),
            pltpu.VMEM((count, 8, LANES), f32),
            dma((4,)), dma((4,)), dma((3, 2)), dma((3, 2)),
            dma((2,)), dma((2,)), dma((2,)), dma((2,)),
            dma((2, count)), dma((2, count)), dma((3,)), dma((3,)),
            dma((2, count)), dma((2, count)), dma((2, count)), dma((2, count)),
            dma((3,)), dma((3,)), dma((count,)), dma((count,)),
        ],
        compiler_params=pltpu.CompilerParams(
            collective_id=0, has_side_effects=True, vmem_limit_bytes=VMEM_BYTES
        ),
        name="layer",
    )(
        layer_input, output_grad, query_weight, key_weight, value_weight, out_weight,
        sink_logit.reshape(1, -1),
    )
    kept = [jax.ShapeDtypeStruct(out.shape, out.dtype) for out in outs[:5]]
    stored = pl.pallas_call(
        store_kernel,
        out_shape=(*kept, jax.ShapeDtypeStruct((1, sink_logit.shape[0]), f32)),
        in_specs=[hbm] * 5 + [vmem],
        out_specs=(hbm,) * 5 + (vmem,),
        scratch_shapes=[pltpu.VMEM(out.shape, out.dtype) for out in kept]
        + [dma((5,)), dma((5,))],
        compiler_params=pltpu.CompilerParams(vmem_limit_bytes=VMEM_BYTES),
        name="store",
    )(*outs)
    return tuple(stored[:5]) + (stored[5].reshape(-1),)


def fits_kernel(mesh, layer_width):
    count, tps = mesh.shape["sp"], mesh.shape["tp"]
    return tps == 4 and count % 8 == 0 and layer_width == count * tps * LANES


def solution(mesh):
    placed = (
        P("sp", "tp"),
        P("sp", "tp"),
        P(None, "tp"),
        P(None, "tp"),
        P(None, "tp"),
        P("tp", None),
        P("tp"),
    )

    def sharded(*arrays):
        width = arrays[0].shape[1]
        body = fused_device if fits_kernel(mesh, width) else per_device
        return jax.shard_map(
            body,
            mesh=mesh,
            in_specs=placed,
            out_specs=(
                P("sp", "tp"),
                P("sp", "tp"),
                P("sp", "tp"),
                P("sp", "tp"),
                P("tp", "sp"),
                P("tp"),
            ),
            check_vma=False,
        )(*arrays)

    return sharded
```

```python
import functools

import jax
import jax.numpy as jnp
from jax import lax
from jax.experimental import pallas as pl
from jax.experimental.pallas import tpu as pltpu
from jax.sharding import PartitionSpec as P

HEADS = 16
KV_HEADS = 8
HEAD = 128
WINDOW = 128


masked_score = -1e30


def extended(cells, sides, width):
    for axis, dim in sides:
        count = lax.axis_size(axis)
        ends = count - 1
        head = lax.slice_in_dim(cells, 0, width, axis=dim)
        tail = lax.slice_in_dim(cells, cells.shape[dim] - width, cells.shape[dim], axis=dim)
        cells = jnp.concatenate(
            [
                lax.ppermute(tail, axis, [(i, (i + 1) % count) for i in range(ends)]),
                cells,
                lax.ppermute(head, axis, [((i + 1) % count, i) for i in range(ends)]),
            ],
            axis=dim,
        )
    return cells


def passed_along(value, axis, steps):
    count = lax.axis_size(axis)
    initial, last = (max(0, -steps), min(count, count - steps))
    return lax.ppermute(value, axis, [(source, source + steps) for source in range(initial, last)])


def contract_rows(left, right):
    return lax.dot_general(
        left, right, (((0,), (0,)), ((), ())), preferred_element_type=jnp.float32
    )


def contract_cols(left, right):
    return lax.dot_general(
        left, right, (((1,), (1,)), ((), ())), preferred_element_type=jnp.float32
    )


def per_device(
    layer_input, output_grad, query_weight, key_weight, value_weight, out_weight, sink_logit
):
    whole_input, whole_grad = (
        lax.all_gather(layer_input, "tp", axis=1, tiled=True),
        lax.all_gather(output_grad, "tp", axis=1, tiled=True),
    )
    tok_rows = whole_input.shape[0]
    query_cols = query_weight.shape[1]
    key_cols = key_weight.shape[1]
    key_heads = key_cols // HEAD
    group_size = HEADS // KV_HEADS
    scaling = HEAD ** (-0.5)
    queries = jnp.dot(whole_input, query_weight, preferred_element_type=jnp.float32).astype(
        jnp.bfloat16
    )
    key_rows = jnp.dot(whole_input, key_weight, preferred_element_type=jnp.float32).astype(
        jnp.bfloat16
    )
    value_rows = jnp.dot(whole_input, value_weight, preferred_element_type=jnp.float32).astype(
        jnp.bfloat16
    )
    out_rows_grad = contract_cols(whole_grad, out_weight).astype(jnp.bfloat16)
    joined = jnp.concatenate([key_rows, value_rows], axis=1)
    band = extended(joined, (("sp", 0),), WINDOW)
    band_rows = band.shape[0]
    band_keys = band[:, :key_cols].reshape(band_rows, key_heads, HEAD)
    band_values = band[:, key_cols:].reshape(band_rows, key_heads, HEAD)
    shard_index = lax.axis_index("sp")
    seq_total = tok_rows * lax.axis_size("sp")
    query_pos = shard_index * tok_rows + jnp.arange(tok_rows, dtype=jnp.int32)
    key_pos = shard_index * tok_rows - WINDOW + jnp.arange(band_rows, dtype=jnp.int32)
    in_window = (
        (jnp.abs(query_pos[:, None] - key_pos[None, :]) <= WINDOW)
        & (key_pos[None, :] >= 0)
        & (key_pos[None, :] < seq_total)
    )
    query_heads = queries.reshape(tok_rows, key_heads, group_size, HEAD)
    grad_heads = out_rows_grad.reshape(tok_rows, key_heads, group_size, HEAD)
    scores = (
        jnp.einsum("qkgd,skd->kgqs", query_heads, band_keys, preferred_element_type=jnp.float32)
        * scaling
    )
    scores = jnp.where(in_window[None, None], scores, masked_score)
    sink_column = sink_logit.reshape(key_heads, group_size)[:, :, None]
    row_max = jnp.maximum(jnp.max(scores, axis=-1), sink_column)
    row_total = jnp.sum(jnp.exp(scores - row_max[..., None]), axis=-1) + jnp.exp(
        sink_column - row_max
    )
    log_total = row_max + jnp.log(row_total)
    soft_weights = jnp.exp(scores - log_total[..., None])
    soft_rounded = soft_weights.astype(jnp.bfloat16)
    attended = jnp.einsum(
        "kgqs,skd->qkgd", soft_rounded, band_values, preferred_element_type=jnp.float32
    ).astype(jnp.bfloat16)
    row_dots = jnp.sum(
        grad_heads.astype(jnp.float32) * attended.astype(jnp.float32), axis=-1
    ).transpose(1, 2, 0)
    prob_grads = jnp.einsum(
        "qkgd,skd->kgqs", grad_heads, band_values, preferred_element_type=jnp.float32
    )
    score_grads = (soft_weights * (prob_grads - row_dots[..., None])).astype(jnp.bfloat16)
    query_grads = (
        jnp.einsum("kgqs,skd->qkgd", score_grads, band_keys, preferred_element_type=jnp.float32)
        * scaling
    )
    query_grads = query_grads.astype(jnp.bfloat16).reshape(tok_rows, query_cols)
    band_key_grads = (
        jnp.einsum("kgqs,qkgd->skd", score_grads, query_heads, preferred_element_type=jnp.float32)
        * scaling
    )
    band_value_grads = jnp.einsum(
        "kgqs,qkgd->skd", soft_rounded, grad_heads, preferred_element_type=jnp.float32
    )
    band_grads = jnp.concatenate(
        [
            band_key_grads.reshape(band_rows, key_cols),
            band_value_grads.reshape(band_rows, key_cols),
        ],
        axis=1,
    )
    sink_part = -jnp.sum(jnp.exp(sink_column - log_total) * row_dots, axis=-1).reshape(-1)
    sink_grad = lax.psum(sink_part, "sp")
    attended_rows = attended.reshape(tok_rows, query_cols)
    input_block = lax.all_to_all(whole_input, "sp", 1, 0, tiled=True)
    grad_block = lax.all_to_all(whole_grad, "sp", 1, 0, tiled=True)
    early_rows = lax.all_gather(
        jnp.concatenate([query_grads, attended_rows], axis=1), "sp", axis=0, tiled=True
    )
    query_part = contract_rows(input_block, early_rows[:, :query_cols])
    out_part = contract_rows(early_rows[:, query_cols:], grad_block)
    returned_low = passed_along(band_grads[:WINDOW].astype(jnp.bfloat16), "sp", -1).astype(
        jnp.float32
    )
    returned_high = passed_along(
        band_grads[band_rows - WINDOW :].astype(jnp.bfloat16), "sp", 1
    ).astype(jnp.float32)
    own_rows = band_grads[WINDOW : WINDOW + tok_rows]
    own_rows = own_rows.at[tok_rows - WINDOW :].add(returned_low)
    own_rows = own_rows.at[:WINDOW].add(returned_high)
    key_grads = own_rows[:, :key_cols].astype(jnp.bfloat16)
    value_grads = own_rows[:, key_cols:].astype(jnp.bfloat16)
    late_rows = lax.all_gather(
        jnp.concatenate([key_grads, value_grads], axis=1), "sp", axis=0, tiled=True
    )
    key_part = contract_rows(input_block, late_rows[:, :key_cols])
    value_part = contract_rows(input_block, late_rows[:, key_cols:])
    partials = (
        contract_cols(query_grads, query_weight)
        + contract_cols(key_grads, key_weight)
        + contract_cols(value_grads, value_weight)
    )
    input_grad = lax.psum_scatter(
        partials.astype(jnp.bfloat16), "tp", scatter_dimension=1, tiled=True
    )
    return (input_grad, query_part, key_part, value_part, out_part, sink_grad)


LANES = 128
MESH = pl.DeviceIdType.MESH
VMEM_BYTES = 60 * 1024 * 1024


def dot_nn(a, b):
    return jnp.dot(a, b, preferred_element_type=jnp.float32)


def layer_kernel(
    x_ref, g_ref, wq_hbm, wk_hbm, wv_hbm, wo_hbm, sink_ref,
    ig_ref, gq_ref, gk_ref, gv_ref, go_ref, sg_ref,
    wq, wk, wv, wo, xg, acc, qs, dos, band, bg, ret_out, ret_in,
    blk, acts, probs, part, rs_in, sinks,
    w_sem, own_sem, ag_send, ag_recv, halo_send, halo_recv, ret_send, ret_recv,
    a2a_send, a2a_recv, blk_send, blk_recv, up_sem, down_sem, cross_sem, acts_recv,
    rs_send, rs_recv, sink_send, sink_recv,
):
    bf16 = jnp.bfloat16
    count, tps = lax.axis_size("sp"), lax.axis_size("tp")
    depth = count // 2
    s, t = lax.axis_index("sp"), lax.axis_index("tp")
    z, x = s // 2, s % 2
    y, core = t // 2, t % 2
    partner = y * 2 + (1 - core)
    across = (1 - y) * 2 + core
    diag = (1 - y) * 2 + (1 - core)
    rows, feats = x_ref.shape
    q_cols, k_cols = wq.shape[1], wk.shape[1]
    block_cols = gq_ref.shape[0]
    per_slot = feats // block_cols
    key_heads = k_cols // HEAD
    group = q_cols // k_cols
    scaling = HEAD**-0.5

    def remote(src, dst, send, recv, dev_s, dev_t):
        return pltpu.make_async_remote_copy(
            src_ref=src, dst_ref=dst, send_sem=send, recv_sem=recv,
            device_id=(dev_s, dev_t), device_id_type=MESH,
        )

    weights = [
        pltpu.make_async_copy(src, dst, w_sem.at[i])
        for i, (src, dst) in enumerate(((wq_hbm, wq), (wk_hbm, wk), (wv_hbm, wv), (wo_hbm, wo)))
    ]
    for copy in weights:
        copy.start()
    own = [
        pltpu.make_async_copy(ref, xg.at[t, a], own_sem.at[a])
        for a, ref in enumerate((x_ref, g_ref))
    ]
    for copy in own:
        copy.start()

    barrier = pltpu.get_barrier_semaphore()
    for peer in (partner, across, diag):
        pl.semaphore_signal(barrier, inc=1, device_id=(s, peer), device_id_type=MESH)
    for d in range(1, count):
        pl.semaphore_signal(
            barrier, inc=1, device_id=((s + d) % count, t), device_id_type=MESH
        )
    pl.semaphore_wait(barrier, 3 + count - 1)

    sources = (x_ref, g_ref)
    to_across = [
        remote(sources[a], xg.at[t, a], ag_send.at[0, a], ag_recv.at[0, a], s, across)
        for a in range(2)
    ]
    to_partner = [
        remote(sources[a], xg.at[t, a], ag_send.at[1, a], ag_recv.at[1, a], s, partner)
        for a in range(2)
    ]
    relay = [
        remote(xg.at[across, a], xg.at[across, a], ag_send.at[2, a], ag_recv.at[2, a], s, partner)
        for a in range(2)
    ]
    for copy in to_across + to_partner:
        copy.start()

    def project_input(slot, first):
        cells = xg[slot, 0]
        span = pl.ds(pl.multiple_of(slot * feats, feats), feats)
        at = 0
        for w in (wq, wk, wv):
            cols = w.shape[1]
            term = dot_nn(cells, w[span, :])
            acc[:, at : at + cols] = term if first else acc[:, at : at + cols] + term
            at += cols

    def project_grad(slot, first):
        span = pl.ds(pl.multiple_of(slot * feats, feats), feats)
        term = contract_cols(xg[slot, 1], wo[:, span])
        lo = q_cols + 2 * k_cols
        acc[:, lo:] = term if first else acc[:, lo:] + term

    for copy in own + weights:
        copy.wait()
    project_input(t, True)
    project_grad(t, True)
    to_partner[0].wait_recv()
    project_input(partner, False)
    to_partner[1].wait_recv()
    project_grad(partner, False)
    to_across[0].wait_recv()
    relay[0].start()
    project_input(across, False)
    relay[0].wait_recv()
    project_input(diag, False)

    mid = pl.ds(WINDOW, rows)
    band[mid, :] = acc[:, q_cols : q_cols + 2 * k_cols].astype(bf16)
    qs[...] = acc[:, :q_cols].astype(bf16)
    has_prev, has_next = s > 0, s < count - 1
    prev, nxt = lax.rem(s + count - 1, count), lax.rem(s + 1, count)
    low, high = pl.ds(0, WINDOW), pl.ds(WINDOW + rows, WINDOW)
    tail_copy = remote(
        band.at[pl.ds(rows, WINDOW)], band.at[low], halo_send.at[0], halo_recv.at[0], nxt, t
    )
    head_copy = remote(
        band.at[pl.ds(WINDOW, WINDOW)], band.at[high], halo_send.at[1], halo_recv.at[1], prev, t
    )

    @pl.when(has_next)
    def _():
        tail_copy.start()

    @pl.when(has_prev)
    def _():
        head_copy.start()

    own_blocks, a2a = [], []

    def columns(a, j):
        lane = (j % per_slot) * block_cols + t * LANES
        return xg.at[j // per_slot, a, :, pl.ds(pl.multiple_of(lane, LANES), LANES)]

    def send_columns(a):
        own_blocks.append(
            pltpu.make_async_copy(columns(a, s), blk.at[t, s, a], own_sem.at[2 + a])
        )
        own_blocks[-1].start()
        for d in range(1, count):
            j = (s + d) % count
            a2a.append(
                remote(
                    columns(a, j), blk.at[t, s, a], a2a_send.at[a, d], a2a_recv.at[a, d], j, t
                )
            )
            a2a[-1].start()

    send_columns(0)
    @pl.when(jnp.logical_not(has_prev))
    def _():
        band[low, :] = jnp.zeros((WINDOW, 2 * k_cols), bf16)

    @pl.when(jnp.logical_not(has_next))
    def _():
        band[high, :] = jnp.zeros((WINDOW, 2 * k_cols), bf16)

    @pl.when(has_prev)
    def _():
        tail_copy.wait_recv()

    @pl.when(has_next)
    def _():
        head_copy.wait_recv()

    band_rows = rows + 2 * WINDOW
    q_at = lax.broadcasted_iota(jnp.int32, (rows, band_rows), 0)
    k_at = lax.broadcasted_iota(jnp.int32, (rows, band_rows), 1) - WINDOW
    k_pos = k_at + s * rows
    in_window = (
        (jnp.abs(q_at - k_at) <= WINDOW) & (k_pos >= 0) & (k_pos < rows * count)
    )
    sink_shares = []
    for h in range(key_heads * group):
        kh = h // group
        cols = slice(h * HEAD, (h + 1) * HEAD)
        keys = band[:, kh * HEAD : (kh + 1) * HEAD]
        values = band[:, k_cols + kh * HEAD : k_cols + (kh + 1) * HEAD]
        scores = jnp.where(in_window, contract_cols(qs[:, cols], keys) * scaling, masked_score)
        sink = sink_ref[0, h]
        top = jnp.maximum(jnp.max(scores, axis=1, keepdims=True), sink)
        e = jnp.exp(scores - top)
        sink_e = jnp.exp(sink - top)
        inverse = 1.0 / (jnp.sum(e, axis=1, keepdims=True) + sink_e)
        p = e * inverse
        probs[h] = p
        sink_shares.append(sink_e * inverse)
        acts[0, s, :, cols] = dot_nn(p.astype(bf16), values).astype(bf16)
    has_up, has_down = z < depth - 1, z > 0
    up, down, other = (z + 1) % depth * 2 + x, (z + depth - 1) % depth * 2 + x, z * 2 + (1 - x)

    def acts_copy(a, block, sems, dev):
        ref = acts.at[a, block]
        return remote(ref, ref, sems.at[a, block], acts_recv.at[a, block], dev, t)

    def send_own(a):
        acts_copy(a, s, cross_sem, other).start()

        @pl.when(has_up)
        def _():
            acts_copy(a, s, up_sem, up).start()

        @pl.when(has_down)
        def _():
            acts_copy(a, s, down_sem, down).start()

    def forward(d, a):
        lower, upper = (z + depth - d) % depth * 2 + x, (z + d) % depth * 2 + x

        @pl.when(z >= d)
        def _():
            acts_copy(a, lower, up_sem, up).wait_recv()
            acts_copy(a, lower, cross_sem, other).start()

            @pl.when(has_up)
            def _():
                acts_copy(a, lower, up_sem, up).start()

        @pl.when(z + d < depth)
        def _():
            acts_copy(a, upper, down_sem, down).wait_recv()
            acts_copy(a, upper, cross_sem, other).start()

            @pl.when(has_down)
            def _():
                acts_copy(a, upper, down_sem, down).start()

    send_own(0)
    to_across[1].wait_recv()
    relay[1].start()
    project_grad(across, False)
    relay[1].wait_recv()
    project_grad(diag, False)
    dos[...] = acc[:, q_cols + 2 * k_cols :].astype(bf16)

    send_columns(1)

    lane_at = lax.broadcasted_iota(jnp.int32, (8, LANES), 1)
    sink_row = jnp.zeros((8, LANES), jnp.float32)
    for kh in range(key_heads):
        keys = band[:, kh * HEAD : (kh + 1) * HEAD]
        values = band[:, k_cols + kh * HEAD : k_cols + (kh + 1) * HEAD]
        key_sum = value_sum = None
        for g in range(group):
            h = kh * group + g
            cols = slice(h * HEAD, (h + 1) * HEAD)
            q, do, p = qs[:, cols], dos[:, cols], probs[h]
            attended = acts[0, s, :, cols]
            dots = jnp.sum(
                do.astype(jnp.float32) * attended.astype(jnp.float32), axis=1, keepdims=True
            )
            ds = (p * (contract_cols(do, values) - dots)).astype(bf16)
            acts[1, s, :, cols] = (dot_nn(ds, keys) * scaling).astype(bf16)
            kg, vg = contract_rows(ds, q), contract_rows(p.astype(bf16), do)
            key_sum = kg if g == 0 else key_sum + kg
            value_sum = vg if g == 0 else value_sum + vg
            total = -jnp.sum(sink_shares[h] * dots)
            sink_row = jnp.where(lane_at == h, total, sink_row)
        bg[:, kh * HEAD : (kh + 1) * HEAD] = key_sum * scaling
        bg[:, k_cols + kh * HEAD : k_cols + (kh + 1) * HEAD] = value_sum
    sinks[s] = sink_row
    ret_out[0] = bg[low, :].astype(bf16)
    ret_out[1] = bg[high, :].astype(bf16)
    to_prev = remote(ret_out.at[0], ret_in.at[0], ret_send.at[0], ret_recv.at[0], prev, t)
    to_next = remote(ret_out.at[1], ret_in.at[1], ret_send.at[1], ret_recv.at[1], nxt, t)

    @pl.when(has_prev)
    def _():
        to_prev.start()

    @pl.when(has_next)
    def _():
        to_next.start()

    send_own(1)
    sink_copies = []
    for d in range(1, count):
        sink_copies.append(
            remote(
                sinks.at[s], sinks.at[s], sink_send.at[d], sink_recv.at[d], (s + d) % count, t
            )
        )
        sink_copies[-1].start()

    tail, head = pl.ds(WINDOW + rows - WINDOW, WINDOW), pl.ds(WINDOW, WINDOW)

    @pl.when(has_next)
    def _():
        to_prev.wait_recv()
        bg[tail, :] = bg[tail, :] + ret_in[0].astype(jnp.float32)

    @pl.when(has_prev)
    def _():
        to_next.wait_recv()
        bg[head, :] = bg[head, :] + ret_in[1].astype(jnp.float32)

    forward(1, 0)
    acts[2, s] = bg[mid, :].astype(bf16)
    send_own(2)

    for copy in own_blocks:
        copy.wait()
    for copy in a2a:
        copy.wait_recv()
    blk_across = remote(blk.at[t], blk.at[t], blk_send.at[0], blk_recv.at[0], s, across)
    blk_partner = remote(blk.at[t], blk.at[t], blk_send.at[1], blk_recv.at[1], s, partner)
    blk_relay = remote(blk.at[across], blk.at[across], blk_send.at[2], blk_recv.at[2], s, partner)
    blk_across.start()
    blk_partner.start()
    qg = acts[1, s]
    kg, vg = acts[2, s, :, :k_cols], acts[2, s, :, k_cols:]

    def partial_for(slot):
        span = pl.ds(pl.multiple_of(slot * feats, feats), feats)
        return (
            contract_cols(qg, wq[span, :])
            + contract_cols(kg, wk[span, :])
            + contract_cols(vg, wv[span, :])
        ).astype(bf16)

    rs_copies = []
    for i, peer in enumerate((across, diag, partner)):
        part[i] = partial_for(peer)
        rs_copies.append(
            remote(part.at[i], rs_in.at[i], rs_send.at[i], rs_recv.at[i], s, peer)
        )
        rs_copies[-1].start()

    def consume(block, first=False):
        right = jnp.concatenate([acts[1, block], acts[2, block]], axis=1)
        left = jnp.concatenate([blk[i, block, 0] for i in range(tps)], axis=1)
        grads = jnp.concatenate([blk[i, block, 1] for i in range(tps)], axis=1)
        term = contract_rows(left, right)
        out_term = contract_rows(acts[0, block], grads)
        pieces = (
            (gq_ref, term[:, :q_cols]),
            (gk_ref, term[:, q_cols : q_cols + k_cols]),
            (gv_ref, term[:, q_cols + k_cols :]),
            (go_ref, out_term),
        )
        for ref, value in pieces:
            ref[...] = value if first else ref[...] + value

    def consume_crossed(block_z):
        block = block_z * 2 + (1 - x)
        for a in range(3):
            acts_copy(a, block, cross_sem, other).wait_recv()
        consume(block)

    def consume_far(d):
        lower, upper = (z + depth - d) % depth, (z + d) % depth

        @pl.when(z >= d)
        def _():
            consume(lower * 2 + x)
            consume_crossed(lower)

        @pl.when(z + d < depth)
        def _():
            consume(upper * 2 + x)
            consume_crossed(upper)

    mine = partial_for(t)
    forward(1, 1)
    blk_across.wait_recv()
    blk_relay.start()
    later = [(d, a) for d in range(1, depth) for a in range(3) if d > 1 or a > 1]
    for d, a in sorted(later, key=sum):
        forward(d, a)
    blk_partner.wait_recv()
    blk_relay.wait_recv()
    consume(s, True)
    consume_crossed(z)
    for d in range(1, depth):
        consume_far(d)
    for copy in rs_copies:
        copy.wait_recv()
    total = mine.astype(jnp.float32)
    for i in range(3):
        total = total + rs_in[i].astype(jnp.float32)
    ig_ref[...] = total.astype(bf16)
    for copy in sink_copies:
        copy.wait_recv()
    sink_total = sinks[0]
    for i in range(1, count):
        sink_total = sink_total + sinks[i]
    sg_ref[...] = sink_total

    for copy in to_across + to_partner + relay + a2a + rs_copies + sink_copies:
        copy.wait_send()
    for copy in (blk_across, blk_partner, blk_relay):
        copy.wait_send()

    @pl.when(has_next)
    def _():
        tail_copy.wait_send()
        to_next.wait_send()

    @pl.when(has_prev)
    def _():
        head_copy.wait_send()
        to_prev.wait_send()

    for a in range(3):
        acts_copy(a, s, cross_sem, other).wait_send()

        @pl.when(has_up)
        def _():
            acts_copy(a, s, up_sem, up).wait_send()

        @pl.when(has_down)
        def _():
            acts_copy(a, s, down_sem, down).wait_send()

        for d in range(1, depth):
            lower, upper = (z + depth - d) % depth * 2 + x, (z + d) % depth * 2 + x

            @pl.when(z >= d)
            def _():
                acts_copy(a, lower, cross_sem, other).wait_send()

                @pl.when(has_up)
                def _():
                    acts_copy(a, lower, up_sem, up).wait_send()

            @pl.when(z + d < depth)
            def _():
                acts_copy(a, upper, cross_sem, other).wait_send()

                @pl.when(has_down)
                def _():
                    acts_copy(a, upper, down_sem, down).wait_send()


def store_kernel(*refs):
    ins, sink_in, outs, sink_out = refs[:5], refs[5], refs[6:11], refs[11]
    held, in_sem, out_sem = refs[12:17], refs[17], refs[18]
    loads = [pltpu.make_async_copy(ins[i], held[i], in_sem.at[i]) for i in range(5)]
    stores = [pltpu.make_async_copy(held[i], outs[i], out_sem.at[i]) for i in range(5)]
    for load in loads:
        load.start()
    sink_out[...] = sink_in[0:1, : sink_out.shape[1]]
    for load, store in zip(loads, stores):
        load.wait()
        store.start()
    for store in stores:
        store.wait()


def fused_device(
    layer_input, output_grad, query_weight, key_weight, value_weight, out_weight, sink_logit
):
    bf16, f32 = jnp.bfloat16, jnp.float32
    count, tps = lax.axis_size("sp"), lax.axis_size("tp")
    rows, feats = layer_input.shape
    width = query_weight.shape[0]
    q_cols, k_cols = query_weight.shape[1], key_weight.shape[1]
    block_cols = width // count
    vmem = pl.BlockSpec(memory_space=pltpu.VMEM)
    hbm = pl.BlockSpec(memory_space=pl.ANY)
    dma = pltpu.SemaphoreType.DMA
    outs = pl.pallas_call(
        layer_kernel,
        out_shape=(
            jax.ShapeDtypeStruct((rows, feats), bf16),
            jax.ShapeDtypeStruct((block_cols, q_cols), f32),
            jax.ShapeDtypeStruct((block_cols, k_cols), f32),
            jax.ShapeDtypeStruct((block_cols, k_cols), f32),
            jax.ShapeDtypeStruct((q_cols, block_cols), f32),
            jax.ShapeDtypeStruct((8, LANES), f32),
        ),
        in_specs=[vmem, vmem, hbm, hbm, hbm, hbm, pl.BlockSpec(memory_space=pltpu.SMEM)],
        out_specs=(vmem,) * 6,
        scratch_shapes=[
            pltpu.VMEM(query_weight.shape, bf16),
            pltpu.VMEM(key_weight.shape, bf16),
            pltpu.VMEM(value_weight.shape, bf16),
            pltpu.VMEM(out_weight.shape, bf16),
            pltpu.VMEM((tps, 2, rows, feats), bf16),
            pltpu.VMEM((rows, 2 * q_cols + 2 * k_cols), f32),
            pltpu.VMEM((rows, q_cols), bf16),
            pltpu.VMEM((rows, q_cols), bf16),
            pltpu.VMEM((rows + 2 * WINDOW, 2 * k_cols), bf16),
            pltpu.VMEM((rows + 2 * WINDOW, 2 * k_cols), f32),
            pltpu.VMEM((2, WINDOW, 2 * k_cols), bf16),
            pltpu.VMEM((2, WINDOW, 2 * k_cols), bf16),
            pltpu.VMEM((tps, count, 2, rows, LANES), bf16),
            pltpu.VMEM((3, count, rows, q_cols), bf16),
            pltpu.VMEM((q_cols // HEAD, rows, rows + 2 * WINDOW), f32),
            pltpu.VMEM((3, rows, feats), bf16),
            pltpu.VMEM((3, rows, feats), bf16),
            pltpu.VMEM((count, 8, LANES), f32),
            dma((4,)), dma((4,)), dma((3, 2)), dma((3, 2)),
            dma((2,)), dma((2,)), dma((2,)), dma((2,)),
            dma((2, count)), dma((2, count)), dma((3,)), dma((3,)),
            dma((3, count)), dma((3, count)), dma((3, count)), dma((3, count)),
            dma((3,)), dma((3,)), dma((count,)), dma((count,)),
        ],
        compiler_params=pltpu.CompilerParams(
            collective_id=0, has_side_effects=True, vmem_limit_bytes=VMEM_BYTES
        ),
        name="layer",
    )(
        layer_input, output_grad, query_weight, key_weight, value_weight, out_weight,
        sink_logit.reshape(1, -1),
    )
    kept = [jax.ShapeDtypeStruct(out.shape, out.dtype) for out in outs[:5]]
    stored = pl.pallas_call(
        store_kernel,
        out_shape=(*kept, jax.ShapeDtypeStruct((1, sink_logit.shape[0]), f32)),
        in_specs=[hbm] * 5 + [vmem],
        out_specs=(hbm,) * 5 + (vmem,),
        scratch_shapes=[pltpu.VMEM(out.shape, out.dtype) for out in kept]
        + [dma((5,)), dma((5,))],
        compiler_params=pltpu.CompilerParams(vmem_limit_bytes=VMEM_BYTES),
        name="store",
    )(*outs)
    return tuple(stored[:5]) + (stored[5].reshape(-1),)


def fits_kernel(mesh, layer_width):
    count, tps = mesh.shape["sp"], mesh.shape["tp"]
    return tps == 4 and count % 8 == 0 and layer_width == count * tps * LANES


def solution(mesh):
    placed = (
        P("sp", "tp"),
        P("sp", "tp"),
        P(None, "tp"),
        P(None, "tp"),
        P(None, "tp"),
        P("tp", None),
        P("tp"),
    )

    def sharded(*arrays):
        width = arrays[0].shape[1]
        body = fused_device if fits_kernel(mesh, width) else per_device
        return jax.shard_map(
            body,
            mesh=mesh,
            in_specs=placed,
            out_specs=(
                P("sp", "tp"),
                P("sp", "tp"),
                P("sp", "tp"),
                P("sp", "tp"),
                P("tp", "sp"),
                P("tp"),
            ),
            check_vma=False,
        )(*arrays)

    return sharded
```
